256 devices in a mesh: ep: 16 (over y, x), tp: 16 (over z, core).
Axes of the slice: x: 4, y: 4, z: 8, core: 2. Of those that a mesh axis runs over, the one named last changes fastest.
Arguments:
- tokens: bfloat16 [1024, 2048], P('ep', 'tp'), may hold values from -64 to 64
- mixer_gain: float32 [2048], replicated, may hold values from 0.1 to 1.9
- expert_gain: float32 [2048], replicated, may hold values from 0.1 to 1.9
- query_weight: bfloat16 [2048, 1024], P(None, 'tp'), may hold values from -0.125 to 0.125
- key_weight: bfloat16 [2048, 1024], P(None, 'tp'), may hold values from -0.125 to 0.125
- value_weight: bfloat16 [2048, 4, 256], P(None, None, 'tp'), may hold values from -0.125 to 0.125
- outgate_weight: bfloat16 [2048, 4, 256], P(None, None, 'tp'), may hold values from -0.125 to 0.125
- ingate_weight: bfloat16 [2048, 4], replicated, may hold values from -0.125 to 0.125
- forget_weight: bfloat16 [2048, 4], replicated, may hold values from -0.125 to 0.125
- forget_bias: float32 [4], replicated, may hold values from -1 to 4
- mixout_weight: bfloat16 [1024, 2048], replicated, may hold values from -0.1875 to 0.1875
- memory_state: float32 [1024, 4, 256, 256], P('ep', None, 'tp'), may hold values from -0.6 to 0.6
- norm_state: float32 [1024, 4, 256], P('ep'), may hold values from -0.6 to 0.6
- max_state: float32 [1024, 4], P('ep'), may hold values from -4 to 4
- expert_gate: bfloat16 [256, 2048, 256], P(('ep', 'tp')), may hold values from -0.125 to 0.125
- expert_up: bfloat16 [256, 2048, 256], P(('ep', 'tp')), may hold values from -0.125 to 0.125
- expert_down: bfloat16 [256, 256, 2048], P(('ep', 'tp')), may hold values from -0.1875 to 0.1875
- routes: int32 [1024, 2], P('ep'), may hold values from 0 to 63, all different within a row; in each aligned block of 64 rows (0 to 63, 64 to 127, ...) at most 4 rows name the same one
- route_weights: float32 [1024, 2], P('ep'), may hold values from 0.1 to 1
Outputs:
- mixed_out: bfloat16 [1024, 2048], P('ep', 'tp')
- memory_next: float32 [1024, 4, 256, 256], P('ep', None, 'tp')
- norm_next: float32 [1024, 4, 256], P('ep')
- max_next: float32 [1024, 4], P('ep')
The draws below stay inside these ranges and needn't reach their ends.
Inputs may be any that keep to these rules, and one draw needn't show every extreme that they name: `routes`: each row names 2 different experts; in the rows of one index of ep (aligned blocks of 64 rows) no expert is named by more than 4 rows, a bound that some block reaches.
All inputs are finite; a program needn't handle non-finite values.
Results may differ from the reference program's by a relative error of at most 0.0079.
Values may be sent and summed in bfloat16 or wider, within the bound.
No kernel may reach another device: no remote copies, remote signals or barrier semaphores. Data moves between devices by JAX's collectives and lax.ppermute only.
A program may use at most 64 MiB of HBM per device.

```python
import math
import jax
import jax.numpy as jnp
import numpy as np
from jax import lax

D = 2048
HEADS = 4
HEAD_DIM = 256
FF = 1024
FF_SPLIT = 4
TOPK = 2
SEQS = 64
BATCH = 1024
EXPERTS = 64
CAP = 4
N_EP = 16


def draw_tokens(key, part):
    key_base, key_rows = jax.random.split(key, 2)
    column_scale = jnp.exp(jnp.log(4.0) * (jnp.arange(D, dtype=jnp.float32) / D - 0.5))
    base_draw = jnp.clip(jax.random.normal(key_base, (BATCH, D), jnp.float32), -6.0, 6.0)
    row_scale = jnp.exp(jax.random.uniform(key_rows, (BATCH, 1), jnp.float32, jnp.log(0.5), jnp.log(5.0)))
    return (base_draw * column_scale * row_scale).astype(jnp.bfloat16)


def level_of(own_key, shape, cuts, least, high):
    level, own = 1.0, jax.random.fold_in(own_key, 6)
    for dim, blocks in cuts:
        draws = jnp.exp(jax.random.uniform(jax.random.fold_in(own, dim), (blocks,), jnp.float32, least / len(cuts), high / len(cuts)))
        level = level * jnp.repeat(draws, shape[dim] // blocks).reshape([-1 if axis == dim else 1 for axis in range(len(shape))])
    return level


def deal_out(key, own, number, rows, amount, top, limit, lean):
    order = jax.random.permutation(key, amount)
    crowded, common = portions_of(amount, rows * top, limit, lean, True), portions_of(amount, rows * top, limit, lean, False)
    places = jnp.arange(amount)

    def named(lengths, turn):
        used = int((lengths > 0).sum())
        fixed = max(1, used // 4)
        moved = fixed + (places - fixed + turn * (used - fixed)) % max(1, amount - fixed)
        return jnp.zeros((amount,), jnp.int32).at[order[jnp.where(places < fixed, places, moved)]].set(jnp.asarray(lengths, jnp.int32))

    lengths = jnp.where(number % 4 == 0, named(crowded, number // 4), named(common, number - number // 4 - 1))
    mixed = jax.random.permutation(jax.random.fold_in(own, 3), amount)
    giver, sink = mixed[0:amount // 2 * 2:2], mixed[1:amount // 2 * 2:2]
    slack = jnp.minimum(lengths[giver] - 1, limit - lengths[sink]) // 2
    slack = jnp.where((giver == order[0]) | (sink == order[0]) | (lengths[sink] == 0), 0, jnp.maximum(slack, 0))
    moved = jax.random.randint(jax.random.fold_in(own, 4), (amount // 2,), 0, 1 << 20) % (slack + 1)
    lengths = lengths.at[giver].add(-moved).at[sink].add(moved)
    items = jnp.searchsorted(jnp.cumsum(lengths), jnp.arange(rows * top), side="right").astype(jnp.int32)
    listing = items.reshape(top, rows).T
    listing = listing[jax.random.permutation(jax.random.fold_in(own, 1), rows)]
    turn = jax.random.randint(jax.random.fold_in(own, 2), (rows, 1), 0, top)
    return jnp.take_along_axis(listing, (jnp.arange(top)[None, :] + turn) % top, axis=1)


def portions_of(number_of, total, most, slope, full):
    loads = [(1 << 20) // math.isqrt(standing ** slope) + 1 for standing in range(1, number_of + 1)]
    largest = most if full else min(most, max(-(-total // number_of), total * loads[0] // sum(loads)))
    least = 1 if total - largest >= number_of - 1 else 0
    counts, spare = [largest] + [least] * (number_of - 1), total - largest - least * (number_of - 1)
    while spare > 0:
        movable = [i for i in range(1, number_of) if counts[i] < largest] or [i for i in range(1, number_of) if counts[i] < most]
        whole, remaining = sum([loads[i] for i in movable]), spare
        for i in movable:
            addition = min(most - counts[i], max(1, remaining * loads[i] // whole), spare)
            counts[i] = counts[i] + addition
            spare = spare - addition
    return np.array(counts)


def gaussian(rng, shape, scale, bound, cuts=(), held_as=jnp.bfloat16):
    loudness = level_of(rng, shape, cuts, -0.22, 0.18) if cuts else 1.0
    array = jax.random.normal(rng, shape, jnp.float32) * scale * loudness
    return jnp.minimum(jnp.maximum(array, -bound), bound).astype(held_as)


def setup_inputs(seed: int = 0) -> dict:
    seeds = jax.random.split(jax.random.key(seed), 20)
    tokens = draw_tokens(jax.random.fold_in(seeds[19], 71), 0)
    mixer_gain = jnp.clip(1.0 + 0.18 * jax.random.normal(seeds[1], (D,), jnp.float32), 0.1, 1.9)
    expert_gain = jnp.clip(1.0 + 0.18 * jax.random.normal(seeds[2], (D,), jnp.float32), 0.1, 1.9)
    query_weight = gaussian(seeds[3], (D, HEADS * HEAD_DIM), D ** -0.5, 0.125, ((1, 16),))
    key_weight = gaussian(seeds[4], (D, HEADS * HEAD_DIM), D ** -0.5, 0.125, ((1, 16),))
    value_weight = gaussian(seeds[5], (D, HEADS, HEAD_DIM), D ** -0.5, 0.125, ((2, 16),))
    outgate_weight = gaussian(seeds[6], (D, HEADS, HEAD_DIM), D ** -0.5, 0.125, ((2, 16),))
    ingate_weight = gaussian(seeds[7], (D, HEADS), D ** -0.5, 0.125)
    forget_weight = gaussian(seeds[8], (D, HEADS), D ** -0.5, 0.125)
    forget_bias = jnp.clip(jax.random.uniform(seeds[9], (HEADS,), jnp.float32, -1.0, 4.0), -1.0, 4.0)
    mixout_weight = gaussian(seeds[10], (HEADS * HEAD_DIM, D), (HEADS * HEAD_DIM) ** -0.5, 0.1875)
    memory_state = gaussian(seeds[11], (BATCH, HEADS, HEAD_DIM, HEAD_DIM), 0.1, 0.6, ((0, 16), (2, 16)), jnp.float32)
    norm_state = gaussian(seeds[12], (BATCH, HEADS, HEAD_DIM), 0.1, 0.6, ((0, 16),), jnp.float32)
    max_state = gaussian(seeds[13], (BATCH, HEADS), 1.0, 4.0, ((0, 16),), jnp.float32)
    expert_gate = gaussian(seeds[14], (EXPERTS * FF_SPLIT, D, FF // FF_SPLIT), D ** -0.5, 0.125, ((0, 256),))
    expert_up = gaussian(seeds[15], (EXPERTS * FF_SPLIT, D, FF // FF_SPLIT), D ** -0.5, 0.125, ((0, 256),))
    expert_down = gaussian(seeds[16], (EXPERTS * FF_SPLIT, FF // FF_SPLIT, D), FF ** -0.5, 0.1875, ((0, 256),))
    routes_keys = jax.random.split(jax.random.fold_in(seeds[17], 1), BATCH // SEQS)
    routes_turns = jax.random.permutation(jax.random.fold_in(seeds[17], 3), BATCH // SEQS)
    routes = jax.vmap(lambda own, number: deal_out(jax.random.fold_in(seeds[17], 2), own, number, SEQS, EXPERTS, TOPK, CAP, 2))(routes_keys, routes_turns).reshape((BATCH, TOPK))
    route_weights = jnp.clip(jnp.exp(math.log(1.0) - 2.3025851 * jax.random.uniform(seeds[18], (BATCH, TOPK), jnp.float32) ** level_of(seeds[18], (BATCH, TOPK), ((0, 16),), -0.2, 0.2)), 0.1, 1.0)
    return dict(tokens=tokens, mixer_gain=mixer_gain, expert_gain=expert_gain, query_weight=query_weight, key_weight=key_weight, value_weight=value_weight, outgate_weight=outgate_weight, ingate_weight=ingate_weight, forget_weight=forget_weight, forget_bias=forget_bias, mixout_weight=mixout_weight, memory_state=memory_state, norm_state=norm_state, max_state=max_state, expert_gate=expert_gate, expert_up=expert_up, expert_down=expert_down, routes=routes, route_weights=route_weights)


eps = 1e-06

def run_expert(packed):
    row_block, gate_blocks, up_blocks, down_blocks = packed
    block_count, width, block_units = gate_blocks.shape
    gate_mat = jnp.moveaxis(gate_blocks, 0, 1).reshape(width, block_count * block_units)
    up_mat = jnp.moveaxis(up_blocks, 0, 1).reshape(width, block_count * block_units)
    down_mat = down_blocks.reshape(block_count * block_units, down_blocks.shape[2])
    gate_part = jnp.dot(row_block, gate_mat, preferred_element_type=jnp.float32)
    up_part = jnp.dot(row_block, up_mat, preferred_element_type=jnp.float32)
    hidden = (jax.nn.silu(gate_part) * up_part).astype(jnp.bfloat16)
    return jnp.dot(hidden, down_mat, preferred_element_type=jnp.float32).astype(jnp.bfloat16)

def reference(tokens, mixer_gain, expert_gain, query_weight, key_weight, value_weight, outgate_weight, ingate_weight, forget_weight, forget_bias, mixout_weight, memory_state, norm_state, max_state, expert_gate, expert_up, expert_down, routes, route_weights):
    row_count = tokens.shape[0]
    token_float = tokens.astype(jnp.float32)
    inverse = lax.rsqrt(lax.optimization_barrier(jnp.mean(token_float * token_float, axis=1, keepdims=True)) + eps)
    scaled = (token_float * mixer_gain).astype(jnp.bfloat16)
    query_full = (inverse * jnp.dot(scaled, query_weight, preferred_element_type=jnp.float32)).reshape(row_count, HEADS, HEAD_DIM)
    key_full = (inverse * jnp.dot(scaled, key_weight, preferred_element_type=jnp.float32) * HEAD_DIM ** (-0.5)).reshape(row_count, HEADS, HEAD_DIM)
    values = (inverse * jnp.dot(scaled, value_weight.reshape(D, HEADS * HEAD_DIM), preferred_element_type=jnp.float32)).reshape(row_count, HEADS, HEAD_DIM)
    outgate = (inverse * jnp.dot(scaled, outgate_weight.reshape(D, HEADS * HEAD_DIM), preferred_element_type=jnp.float32)).reshape(row_count, HEADS, HEAD_DIM)
    ingate = inverse * jnp.dot(scaled, ingate_weight, preferred_element_type=jnp.float32)
    logforget = jax.nn.log_sigmoid(inverse * jnp.dot(scaled, forget_weight, preferred_element_type=jnp.float32) + forget_bias)
    max_next = jnp.maximum(logforget + max_state, ingate)
    decay_rate = jnp.exp(logforget + max_state - max_next)
    inflow = jnp.exp(ingate - max_next)
    memory_next = decay_rate[:, :, None, None] * memory_state + inflow[:, :, None, None] * values[:, :, :, None] * key_full[:, :, None, :]
    norm_next = decay_rate[:, :, None] * norm_state + inflow[:, :, None] * key_full
    numerator = jnp.einsum('bhvk,bhk->bhv', memory_next, query_full, precision=lax.Precision.HIGHEST)
    denominator = jnp.maximum(jnp.abs(lax.optimization_barrier(jnp.sum(norm_next * query_full, axis=2))), jnp.exp(-max_next))
    gated_heads = (jax.nn.sigmoid(outgate) * (numerator / denominator[:, :, None])).astype(jnp.bfloat16)
    middle = (token_float + jnp.dot(gated_heads.reshape(row_count, HEADS * HEAD_DIM), mixout_weight, preferred_element_type=jnp.float32)).astype(jnp.bfloat16)
    middle_float = middle.astype(jnp.float32)
    inverse_two = lax.rsqrt(lax.optimization_barrier(jnp.mean(middle_float * middle_float, axis=1, keepdims=True)) + eps)
    normed = (middle_float * inverse_two * expert_gain).astype(jnp.bfloat16)
    grouped = routes.reshape(N_EP, SEQS * TOPK)
    onehot = (grouped[:, :, None] == jnp.arange(EXPERTS, dtype=jnp.int32)[None, None, :]).astype(jnp.int32)
    slot_rank = lax.optimization_barrier(jnp.sum(onehot * (jnp.cumsum(onehot, axis=1) - 1), axis=2))
    row_index = (jnp.arange(N_EP, dtype=jnp.int32)[:, None] * CAP + slot_rank).reshape(-1).astype(jnp.int32)
    expert_index = grouped.reshape(-1).astype(jnp.int32)
    token_index = (jnp.arange(row_count * TOPK, dtype=jnp.int32) // TOPK).astype(jnp.int32)
    buffer = jnp.zeros((EXPERTS, N_EP * CAP, D), jnp.bfloat16).at[expert_index, row_index].set(normed[token_index])
    gate_blocks = expert_gate.reshape(EXPERTS, FF_SPLIT, D, FF // FF_SPLIT)
    up_blocks = expert_up.reshape(EXPERTS, FF_SPLIT, D, FF // FF_SPLIT)
    down_blocks = expert_down.reshape(EXPERTS, FF_SPLIT, FF // FF_SPLIT, D)
    results = lax.map(run_expert, (buffer, gate_blocks, up_blocks, down_blocks))
    picked = results[expert_index, row_index].astype(jnp.float32).reshape(row_count, TOPK, D)
    shares = route_weights / lax.optimization_barrier(jnp.sum(route_weights, axis=1, keepdims=True))
    mixed_out = (middle_float + lax.optimization_barrier(jnp.sum(shares[:, :, None] * picked, axis=1))).astype(jnp.bfloat16)
    return (mixed_out, memory_next, norm_next, max_next)
```

```python
import jax
import jax.numpy as jnp
import numpy as np
from jax import lax
from jax.sharding import Mesh
from jax.sharding import PartitionSpec as P

FF_SPLIT = 4
EPS = 1e-06
F32 = jnp.float32
BF16 = jnp.bfloat16


def swap_cores(x):
    return lax.ppermute(x, "core", [(0, 1), (1, 0)])


def spread(shard):
    copies = jnp.broadcast_to(shard, (lax.axis_size("z"), *shard.shape))
    own = lax.all_to_all(copies, "z", 0, 0, tiled=True)
    other = swap_cores(own)
    first = lax.axis_index("core") == 0
    return jnp.where(first, own, other), jnp.where(first, other, own)


def side_by_side(low, high):
    both = jnp.stack([low, high], 1)
    z, two, rows, width = both.shape
    return jnp.transpose(both, (2, 0, 1, 3)).reshape(rows, z * two * width)


def exchange(x):
    return lax.all_to_all(x, ("z", "core", "ep"), 0, 0, tiled=True)


def slot_tables(groups, width):
    t = np.arange(width)[:, None, None]
    g = np.arange(groups)[None, :, None]
    r = np.arange(4)[None, None, :]
    expert = g * (width // FF_SPLIT) + t // FF_SPLIT
    core = t % 2
    send = np.full((width, groups, 4, 3), -1, np.int32)
    for b in range(2):
        slot = (expert * 4 + 2 * core + b)[:, :, 0]
        send[:, :, b, 0] = slot
        send[:, :, 2, 1 + b] = slot
    back = expert * 4 + 2 * ((r // 2) ^ core) + r % 2
    return send.reshape(-1, 3), np.broadcast_to(back, (width, groups, 4)).reshape(-1).astype(np.int32)


def route_targets(routes, expert_count):
    picks = [(routes[:, k : k + 1] == jnp.arange(expert_count, dtype=jnp.int32)).astype(BF16) for k in range(2)]
    rows = routes.shape[0]
    earlier = jnp.tril(jnp.ones((rows, rows), BF16), -1)
    counts = jnp.dot(earlier, picks[0] + picks[1], preferred_element_type=F32)
    return [
        routes[:, k] * 4 + jnp.sum(counts * picks[k].astype(F32), axis=1).astype(jnp.int32) for k in range(2)
    ]


def local(
    tokens,
    mixer_gain,
    expert_gain,
    query_weight,
    key_weight,
    value_weight,
    outgate_weight,
    ingate_weight,
    forget_weight,
    forget_bias,
    mixout_weight,
    memory_state,
    norm_state,
    max_state,
    expert_gate,
    expert_up,
    expert_down,
    routes,
    route_weights,
):
    rows, own_width = tokens.shape
    width = mixer_gain.shape[0]
    heads, head_dim = norm_state.shape[1:]
    local_values = value_weight.shape[2]
    groups = lax.axis_size("ep")
    tp = lax.axis_size("z") * lax.axis_size("core")
    expert_count = groups * tp // FF_SPLIT

    x = side_by_side(*spread(tokens)).astype(F32)
    inverse = lax.rsqrt(jnp.mean(x * x, axis=1, keepdims=True) + EPS)
    scaled = (x * mixer_gain).astype(BF16)

    def project(w):
        return inverse * jnp.dot(scaled, w.reshape(width, -1), preferred_element_type=F32)

    query_own = project(query_weight)
    key_own = project(key_weight) * head_dim ** (-0.5)
    low, high = spread(jnp.concatenate([query_own, key_own], 1))
    own_cols = query_own.shape[1]
    query = side_by_side(low[:, :, :own_cols], high[:, :, :own_cols]).reshape(rows, heads, head_dim)
    key = side_by_side(low[:, :, own_cols:], high[:, :, own_cols:]).reshape(rows, heads, head_dim)
    values = project(value_weight).reshape(rows, heads, local_values)
    outgate = project(outgate_weight).reshape(rows, heads, local_values)
    ingate = project(ingate_weight)
    logforget = jax.nn.log_sigmoid(project(forget_weight) + forget_bias)
    max_next = jnp.maximum(logforget + max_state, ingate)
    decay = jnp.exp(logforget + max_state - max_next)
    inflow = jnp.exp(ingate - max_next)
    memory_next = (
        decay[:, :, None, None] * memory_state
        + inflow[:, :, None, None] * values[:, :, :, None] * key[:, :, None, :]
    )
    norm_next = decay[:, :, None] * norm_state + inflow[:, :, None] * key
    numerator = jnp.sum(memory_next * query[:, :, None, :], axis=3)
    denominator = jnp.maximum(jnp.abs(jnp.sum(norm_next * query, axis=2)), jnp.exp(-max_next))
    gated = (jax.nn.sigmoid(outgate) * (numerator / denominator[:, :, None])).astype(BF16)
    gated = gated.reshape(rows, heads * local_values)

    send_table, back_table = slot_tables(groups, tp)
    targets = route_targets(routes, expert_count)
    wanted = jnp.asarray(send_table)[:, :, None]
    place = ((wanted == targets[0]) | (wanted == targets[1])).astype(BF16).reshape(len(send_table), 3 * rows)
    empty = jnp.zeros_like(gated)
    sources = jnp.concatenate(
        [tokens, jnp.concatenate([gated, empty], 1), jnp.concatenate([empty, gated], 1)], 0
    )
    message = jnp.dot(place, sources, preferred_element_type=F32).astype(BF16)
    arrived = exchange(message.reshape(tp * groups, 4, own_width)).reshape(tp, groups, 4, own_width)

    routed = jnp.transpose(arrived[:, :, :2], (1, 2, 0, 3)).reshape(groups * 2, width).astype(F32)
    recall = arrived[:, :, 2].reshape(tp, groups, 2, heads, local_values)
    recall = jnp.transpose(recall, (1, 2, 3, 0, 4)).reshape(groups * 2, heads * head_dim)
    middle = (routed + jnp.dot(recall, mixout_weight, preferred_element_type=F32)).astype(BF16)
    middle_float = middle.astype(F32)
    inverse_two = lax.rsqrt(jnp.mean(middle_float * middle_float, axis=1, keepdims=True) + EPS)
    normed = (middle_float * inverse_two * expert_gain).astype(BF16)
    others = swap_cores(normed)
    block = jnp.stack([normed.reshape(groups, 2, width), others.reshape(groups, 2, width)], 1)
    block = block.reshape(groups * 4, width)
    gate_part = jnp.dot(block, expert_gate[0], preferred_element_type=F32)
    up_part = jnp.dot(block, expert_up[0], preferred_element_type=F32)
    hidden = (jax.nn.silu(gate_part) * up_part).astype(BF16)
    part = jnp.dot(hidden, expert_down[0], preferred_element_type=F32)
    residual = 0.5 * middle_float.reshape(groups, 1, 2, width)
    residual = jnp.concatenate([residual, jnp.zeros_like(residual)], 1).reshape(groups * 4, width)
    part = (part + residual).astype(BF16)
    part = jnp.transpose(part.reshape(groups, 4, tp, own_width), (2, 0, 1, 3))
    returned = exchange(part.reshape(tp * groups, 4, own_width)).reshape(tp * groups * 4, own_width)

    shares = route_weights / jnp.sum(route_weights, axis=1, keepdims=True)
    mixed = jnp.zeros((rows, own_width), F32)
    for k in range(2):
        pick = (jnp.asarray(back_table)[None, :] == targets[k][:, None]).astype(BF16)
        mixed = mixed + shares[:, k : k + 1] * jnp.dot(pick, returned, preferred_element_type=F32)
    return mixed.astype(BF16), memory_next, norm_next, max_next


def solution(mesh):
    tp = mesh.shape["tp"]
    inner = Mesh(mesh.devices.reshape(mesh.shape["ep"], tp // 2, 2), ("ep", "z", "core"))
    t = ("z", "core")
    every = ("ep", "z", "core")
    in_specs = (
        P("ep", t),
        P(),
        P(),
        P(None, t),
        P(None, t),
        P(None, None, t),
        P(None, None, t),
        P(),
        P(),
        P(),
        P(),
        P("ep", None, t, None),
        P("ep", None, None),
        P("ep", None),
        P(every, None, None),
        P(every, None, None),
        P(every, None, None),
        P("ep", None),
        P("ep", None),
    )
    out_specs = (P("ep", t), P("ep", None, t, None), P("ep", None, None), P("ep", None))
    return jax.shard_map(local, mesh=inner, in_specs=in_specs, out_specs=out_specs, check_vma=False)
```

```python
import jax
import jax.numpy as jnp
from jax import lax
from jax.experimental import pallas as pl
from jax.experimental.pallas import tpu as pltpu
from jax.sharding import Mesh
from jax.sharding import PartitionSpec as P

EPS = 1e-06
F32 = jnp.float32
BF16 = jnp.bfloat16


def swap_cores(x):
    return lax.ppermute(x, "core", [(0, 1), (1, 0)])


def gather_z(copies):
    own = lax.all_to_all(copies, "z", 0, 0, tiled=True)
    return own, swap_cores(own)


def exchange(x):
    return lax.all_to_all(x, ("z", "core", "ep"), 0, 0, tiled=True)


def hbm(x):
    return pltpu.with_memory_space_constraint(x, pltpu.HBM)


VMEM = pl.BlockSpec(memory_space=pltpu.VMEM)
SMEM = pl.BlockSpec(memory_space=pltpu.SMEM)
HBM = pl.BlockSpec(memory_space=pltpu.HBM)


def room(mib):
    return pltpu.CompilerParams(vmem_limit_bytes=mib * 1024 * 1024)


def shape(dims, dtype=F32):
    return jax.ShapeDtypeStruct(dims, dtype)


def dot(a, b):
    return jnp.dot(a, b, preferred_element_type=F32)


def dot_t(a, b):
    return lax.dot_general(a, b, (((1,), (1,)), ((), ())), preferred_element_type=F32)


def diagonal(n):
    return lax.broadcasted_iota(jnp.int32, (n, n), 0) == lax.broadcasted_iota(jnp.int32, (n, n), 1)


def as_row(column):
    return jnp.sum(jnp.where(diagonal(column.shape[0]), column, 0.0), axis=0, keepdims=True)


def low_lanes(rows):
    return lax.broadcasted_iota(jnp.int32, (rows, 128), 1) < 64


def prepare_kernel(
    routes, weights, wq, wk, wv, wo, gain, state, wi, wf, wqk, wvo, gain_out, state_out, wg, columns, rows, sems
):
    half = wq.shape[0]
    copies = [
        pltpu.make_async_copy(src, dst.at[pl.ds(at, half)], sems.at[n])
        for n, (src, dst, at) in enumerate(((wq, wqk, 0), (wk, wqk, half), (wv, wvo, 0), (wo, wvo, half)))
    ]
    copies.append(pltpu.make_async_copy(gain, gain_out, sems.at[4]))
    copies.append(pltpu.make_async_copy(state, state_out, sems.at[5]))
    for copy in copies:
        copy.start()
    wg[...] = jnp.concatenate([wi[...].astype(F32), wf[...].astype(F32)], axis=0).astype(BF16)
    count = routes.shape[0]
    at_row = lax.broadcasted_iota(jnp.int32, (count, count), 0)
    at_column = lax.broadcasted_iota(jnp.int32, (count, count), 1)
    named = [(routes[:, k : k + 1] == at_column).astype(F32) for k in range(2)]
    earlier = (at_column < at_row).astype(F32)
    counts = dot(earlier.astype(BF16), (named[0] + named[1]).astype(BF16))
    total = weights[:, :1] + weights[:, 1:]
    lane = lax.broadcasted_iota(jnp.int32, (count, 128), 1)
    out = jnp.zeros((count, 128), F32)
    for k in range(2):
        rank = jnp.sum(counts * named[k], axis=1, keepdims=True)
        target = (routes[:, k : k + 1] * 4).astype(F32) + rank
        out = jnp.where(lane == k, target, out)
        out = jnp.where(lane == 2 + k, weights[:, k : k + 1] / total, out)
        rows[pl.ds(k, 1), :] = twice(as_row(target))
    columns[...] = out
    for copy in copies:
        copy.wait()


def project_kernel(
    first, own, other, gain, wqk, wvo, wg, bias, state, payload, values, gates, most, floor, decay, inflow
):
    even = first[0] == 0
    rows = own.shape[1]
    acc_qk = jnp.zeros((rows, 128), F32)
    acc_vo = jnp.zeros((128, rows), F32)
    acc_g = jnp.zeros((8, rows), F32)
    squares = jnp.zeros((rows, 128), F32)
    for z in range(own.shape[0]):
        a = own[z].astype(F32)
        b = other[z].astype(F32)
        x = jnp.concatenate([jnp.where(even, a, b), jnp.where(even, b, a)], axis=1)
        squares = squares + x[:, :128] * x[:, :128] + x[:, 128:] * x[:, 128:]
        at = pl.ds(z * 256, 256)
        scaled = (x * gain[:, at]).astype(BF16)
        acc_qk = acc_qk + dot_t(scaled, wqk[:, at])
        acc_vo = acc_vo + dot_t(wvo[:, at], scaled)
        acc_g = acc_g + dot_t(wg[:, at], scaled)
    mean = jnp.sum(squares, axis=1, keepdims=True) * (1.0 / (own.shape[0] * 256))
    inverse = lax.rsqrt(mean + EPS)
    inverse_row = as_row(inverse)
    scale = jnp.where(low_lanes(rows), 1.0, 256.0 ** (-0.5))
    out = acc_qk * inverse * scale
    for z in range(own.shape[0]):
        payload[z] = out
    acc_vo = acc_vo * inverse_row
    values[...] = acc_vo[:64]
    gates[...] = jax.nn.sigmoid(acc_vo[64:])
    acc_g = acc_g * inverse_row
    ingate = acc_g[:4]
    forget = acc_g[4:] + bias[...]
    logforget = jnp.minimum(forget, 0.0) - jnp.log1p(jnp.exp(-jnp.abs(forget)))
    carried = logforget + state[...]
    top = jnp.maximum(carried, ingate)
    most[...] = top
    floor[...] = jnp.exp(-top)
    decay[...] = jnp.exp(carried - top)
    inflow[...] = jnp.exp(ingate - top)


def twice(x):
    return jnp.concatenate([x, x], axis=1)


def recall_kernel(
    first, own, other, values, gates, floor, decay, inflow, targets, norm_hbm, tokens_hbm, memory, message, keys,
    queries, norm, tokens, state, staged, outgoing, sems, in_sems, out_sems,
):
    heads = 4
    rows = own.shape[1]
    block = 8

    def fetch(i):
        at = pl.ds(i * block, block)
        return pltpu.make_async_copy(memory.at[at], state.at[at], sems.at[i])

    for i in range(rows // block):
        fetch(i).start()
    norm_copy = pltpu.make_async_copy(norm_hbm, norm, in_sems.at[0])
    norm_copy.start()
    tokens_copy = pltpu.make_async_copy(tokens_hbm, tokens, in_sems.at[1])
    tokens_copy.start()
    even = first[0] == 0
    low = low_lanes(rows)
    for z in range(own.shape[0]):
        a = own[z]
        b = other[z]
        e = jnp.where(even, a, b)
        o = jnp.where(even, b, a)
        at = pl.ds(z * 128, 128)
        queries[:, at] = jnp.where(low, e, pltpu.roll(o, 64, 1))
        staged[:, at] = jnp.where(low, pltpu.roll(e, 64, 1), o)
    key_copy = pltpu.make_async_copy(staged, keys, out_sems.at[0])
    key_copy.start()
    lane = lax.broadcasted_iota(jnp.int32, (16, 128), 1) % 64

    def step(i, sums):
        fetch(i).wait()
        sums = list(sums)
        for j in range(block):
            s = i * block + j
            here = lane == s
            for h in range(heads):
                prod = state[s, h] * queries[pl.ds(s, 1), pl.ds(h * 256, 256)]
                total = jnp.sum(prod[:, :128] + prod[:, 128:], axis=1, keepdims=True)
                sums[h] = jnp.where(here, total, sums[h])
        return tuple(sums)

    sums = lax.fori_loop(0, rows // block, step, (jnp.zeros((16, 128), F32),) * heads)
    norm_copy.wait()
    tokens_copy.wait()
    half = lax.broadcasted_iota(jnp.int32, (16, 128), 1) < 64
    upper, lower = [], []
    for h in range(heads):
        at = pl.ds(h * 256, 256)
        q = queries[:, at]
        nq = as_row(jnp.sum(norm[:, h, :] * q, axis=1, keepdims=True))
        kq = as_row(jnp.sum(staged[:, at] * q, axis=1, keepdims=True))
        here = pl.ds(h, 1)
        bottom = jnp.abs(decay[here, :] * nq + inflow[here, :] * kq)
        bottom = jnp.maximum(bottom, floor[here, :])
        kept = twice(decay[here, :] / bottom)
        fresh = twice(inflow[here, :] * kq / bottom)
        mine = pl.ds(h * 16, 16)
        gated = twice(gates[mine, :]) * (kept * sums[h] + fresh * twice(values[mine, :]))
        upper.append(jnp.where(half, gated, 0.0))
        lower.append(jnp.where(half, 0.0, gated))
    both = jnp.concatenate(upper + lower, axis=0).astype(BF16)
    count = outgoing.shape[1]
    row = lax.broadcasted_iota(jnp.int32, (count, 128), 0)
    kind = lax.broadcasted_iota(jnp.int32, (count, 128), 1) // 64
    sends = []
    for part in range(outgoing.shape[0]):
        base = (row // 4) * 16 + 2 * part
        r = row % 4
        slot = jnp.where(r == 2, base + kind, -1).astype(F32)
        picked = jnp.where((slot == targets[:1, :]) | (slot == targets[1:2, :]), 1.0, 0.0)
        slot = jnp.where(r < 2, base + r, -1)[:, :64].astype(F32)
        copied = jnp.where((slot == targets[:1, :64]) | (slot == targets[1:2, :64]), 1.0, 0.0)
        out = dot_t(picked.astype(BF16), both) + dot(copied.astype(BF16), tokens[...])
        outgoing[part] = out.astype(BF16)
        j, c = part // 2, part % 2
        for twin in range(2):
            send = pltpu.make_async_copy(
                outgoing.at[part], message.at[4 * j + 2 * twin + c], out_sems.at[1 + 2 * part + twin]
            )
            send.start()
            sends.append(send)
    for send in sends:
        send.wait()
    key_copy.wait()


def update_kernel(decay_scalar, values, decay, inflow, keys, norm, memory, memory_next, norm_next):
    step = pl.program_id(0)
    heads = 4
    rows = keys.shape[0]

    @pl.when(step == 0)
    def _():
        eye = diagonal(rows)
        for h in range(heads):
            here = pl.ds(h, 1)
            kept = jnp.sum(jnp.where(eye, decay[here, :], 0.0), axis=1, keepdims=True)
            fresh = jnp.sum(jnp.where(eye, inflow[here, :], 0.0), axis=1, keepdims=True)
            norm_next[:, h, :] = kept * norm[:, h, :] + fresh * keys[:, pl.ds(h * 256, 256)]

    block = memory.shape[0]
    lane = lax.broadcasted_iota(jnp.int32, (16, rows), 1)
    fresh = [values[pl.ds(h * 16, 16), :] * inflow[pl.ds(h, 1), :] for h in range(heads)]
    for j in range(block):
        s = step * block + j
        for h in range(heads):
            column = jnp.sum(jnp.where(lane == s, fresh[h], 0.0), axis=1, keepdims=True)
            key = keys[pl.ds(s, 1), pl.ds(h * 256, 256)]
            memory_next[j, h] = decay_scalar[h, s] * memory[j, h] + column * key


def middle_kernel(arrived, mixout, gain, normed, middle, wide, staged, sems):
    count, groups = arrived.shape[0], arrived.shape[1] // 4

    def fetch(m, h):
        source = mixout.at[pl.ds(h * 256 + m * 64, 64)]
        return pltpu.make_async_copy(source, staged.at[m, pl.ds(h * 64, 64)], sems.at[m, h])

    for m in range(count // 4):
        for h in range(4):
            fetch(m, h).start()
    for t in range(count):
        wide[t] = arrived[t].astype(F32)
    low = low_lanes(groups)
    total = jnp.zeros((2 * groups, gain.shape[1]), F32)
    for m in range(count // 4):
        parts, weights = [], []
        for z in range(2):
            t = 4 * m + 2 * z
            e = wide[t, pl.ds(2, groups, stride=4)]
            o = wide[t + 1, pl.ds(2, groups, stride=4)]
            front = jnp.where(low, e, pltpu.roll(o, 64, 1))
            back = jnp.where(low, pltpu.roll(e, 64, 1), o)
            parts.append(jnp.concatenate([front, back], axis=0).astype(BF16))
            for u in range(2):
                for h in range(4):
                    weights.append((h, 2 * z + u))
        for h in range(4):
            fetch(m, h).wait()
        weights = [staged[m, pl.ds(h * 64 + n * 16, 16), :] for h, n in weights]
        total = total + dot(jnp.concatenate(parts, axis=1), jnp.concatenate(weights, axis=0))
    pieces = []
    squares = jnp.zeros((2 * groups, 128), F32)
    for t in range(count):
        rows = [wide[t, pl.ds(b, groups, stride=4)] for b in range(2)]
        piece = jnp.concatenate(rows, axis=0) + total[:, t * 128 : (t + 1) * 128]
        piece = piece.astype(BF16)
        middle[:, pl.ds(t * 128, 128)] = piece
        piece = piece.astype(F32)
        squares = squares + piece * piece
        pieces.append(piece)
    mean = jnp.sum(squares, axis=1, keepdims=True) * (1.0 / gain.shape[1])
    inverse = lax.rsqrt(mean + EPS)
    for t in range(count):
        at = pl.ds(t * 128, 128)
        normed[:, at] = (pieces[t] * inverse * gain[:, at]).astype(BF16)


def expert_kernel(own, other, middle, gate, up, down_hbm, out, wide, down, sem):
    down_copy = pltpu.make_async_copy(down_hbm, down, sem)
    down_copy.start()
    half = own.shape[0]
    groups = half // 2
    rows = jnp.concatenate([own[...], other[...]], axis=0)
    g = dot(rows, gate[0])
    u = dot(rows, up[0])
    hidden = (g * jax.nn.sigmoid(g) * u).astype(BF16)
    down_copy.wait()
    part = dot(hidden, down[0])
    for n in range(4):
        piece = part[n * groups : (n + 1) * groups]
        if n < 2:
            piece = piece + 0.5 * middle[pl.ds(n * groups, groups), :].astype(F32)
        for t in range(out.shape[0]):
            wide[t, pl.ds(n, groups, stride=4)] = piece[:, t * 128 : (t + 1) * 128]
    for t in range(out.shape[0]):
        out[t] = wide[t].astype(BF16)


def finish_kernel(returned, columns, out):
    rows, count = columns.shape[0], returned.shape[0]
    q = lax.broadcasted_iota(jnp.int32, (1, count), 1)
    t, g, r = q // 64, (q // 4) % 16, q % 4
    odd = t % 2
    high = r // 2
    slot = (g * 4 + t // 4) * 4 + 2 * (high + odd - 2 * high * odd) + r % 2
    slot = jnp.broadcast_to(slot.astype(F32), (rows, count))
    total = jnp.zeros((rows, out.shape[1]), F32)
    for k in range(2):
        pick = jnp.where(slot == columns[:, k : k + 1], 1.0, 0.0).astype(BF16)
        total = total + columns[:, 2 + k : 3 + k] * dot(pick, returned[...])
    out[...] = total.astype(BF16)


def local(
    tokens,
    mixer_gain,
    expert_gain,
    query_weight,
    key_weight,
    value_weight,
    outgate_weight,
    ingate_weight,
    forget_weight,
    forget_bias,
    mixout_weight,
    memory_state,
    norm_state,
    max_state,
    expert_gate,
    expert_up,
    expert_down,
    routes,
    route_weights,
):
    rows, own_width = tokens.shape
    width = mixer_gain.shape[0]
    heads, head_dim = norm_state.shape[1:]
    local_values = value_weight.shape[2]
    groups = lax.axis_size("ep")
    tp = lax.axis_size("z") * lax.axis_size("core")
    first = lax.axis_index("core").astype(jnp.int32).reshape(1)
    z = lax.axis_size("z")
    channels = heads * local_values
    features = heads * head_dim

    own, other = gather_z(jnp.broadcast_to(tokens, (z, rows, own_width)))
    turned = [query_weight.T, key_weight.T]
    turned += [jnp.transpose(w, (1, 2, 0)).reshape(channels, width) for w in (value_weight, outgate_weight)]
    turned += [mixer_gain.reshape(1, width), max_state.T]
    wqk, wvo, gain, state, wg, columns, targets = pl.pallas_call(
        prepare_kernel,
        out_shape=[
            shape((2 * channels, width), BF16),
            shape((2 * channels, width), BF16),
            shape((1, width)),
            shape((heads, rows)),
            shape((2 * heads, width), BF16),
            shape((rows, 128)),
            shape((2, 128)),
        ],
        in_specs=[VMEM] * 2 + [HBM] * 6 + [VMEM] * 2,
        out_specs=[VMEM] * 7,
        scratch_shapes=[pltpu.SemaphoreType.DMA((6,))],
        compiler_params=room(4),
        name="prepare",
    )(routes, route_weights, *(hbm(w) for w in turned), ingate_weight.T, forget_weight.T)
    flat = (channels, rows)
    per_head = (heads, rows)
    payload, values, gates, most, floor, decay, inflow = pl.pallas_call(
        project_kernel,
        out_shape=[shape((z, rows, 128)), shape(flat), shape(flat)] + [shape(per_head)] * 4,
        in_specs=[SMEM] + [VMEM] * 8,
        out_specs=[VMEM] * 7,
        compiler_params=room(4),
        name="project",
    )(first, own, other, gain, wqk, wvo, wg, forget_bias.reshape(heads, 1), state)

    own, other = gather_z(payload)
    message, keys = pl.pallas_call(
        recall_kernel,
        out_shape=[pltpu.HBM((tp, groups * 4, own_width), BF16), pltpu.HBM((rows, features), F32)],
        in_specs=[SMEM] + [VMEM] * 8 + [HBM] * 3,
        out_specs=[HBM] * 2,
        scratch_shapes=[
            pltpu.VMEM((rows, features), F32),
            pltpu.VMEM((rows, heads, head_dim), F32),
            pltpu.VMEM((rows, own_width), BF16),
            pltpu.VMEM((rows, heads, local_values, head_dim), F32),
            pltpu.VMEM((rows, features), F32),
            pltpu.VMEM((tp // 2, groups * 4, own_width), BF16),
            pltpu.SemaphoreType.DMA((rows // 8,)),
            pltpu.SemaphoreType.DMA((2,)),
            pltpu.SemaphoreType.DMA((1 + tp,)),
        ],
        compiler_params=room(10),
        name="recall",
    )(
        first, own, other, values, gates, floor, decay, inflow, targets,
        hbm(norm_state), hbm(tokens), hbm(memory_state),
    )
    arrived = exchange(message.reshape(tp * groups, 4, own_width)).reshape(tp, groups * 4, own_width)

    block = 8
    blocked = pl.BlockSpec((block, heads, local_values, head_dim), lambda i: (i, 0, 0, 0))
    memory_next, norm_next = pl.pallas_call(
        update_kernel,
        grid=(rows // block,),
        out_shape=[shape(memory_state.shape), shape(norm_state.shape)],
        in_specs=[SMEM] + [VMEM] * 5 + [blocked],
        out_specs=[blocked, VMEM],
        compiler_params=room(8),
        name="update",
    )(decay, values, decay, inflow, keys, norm_state, hbm(memory_state))

    normed, middle = pl.pallas_call(
        middle_kernel,
        out_shape=[shape((groups * 2, width), BF16)] * 2,
        in_specs=[VMEM, HBM, VMEM],
        out_specs=[VMEM] * 2,
        scratch_shapes=[
            pltpu.VMEM((tp, groups * 4, own_width), F32),
            pltpu.VMEM((4, features // 4, width), BF16),
            pltpu.SemaphoreType.DMA((4, 4)),
        ],
        compiler_params=room(12),
        name="middle",
    )(arrived, hbm(mixout_weight), expert_gain.reshape(1, width))
    part = pl.pallas_call(
        expert_kernel,
        out_shape=shape((tp, groups * 4, own_width), BF16),
        in_specs=[VMEM] * 5 + [HBM],
        out_specs=VMEM,
        scratch_shapes=[
            pltpu.VMEM((tp, groups * 4, own_width), F32),
            pltpu.VMEM(expert_down.shape, BF16),
            pltpu.SemaphoreType.DMA,
        ],
        compiler_params=room(6),
        name="expert",
    )(normed, swap_cores(normed), middle, expert_gate, expert_up, hbm(expert_down))
    returned = exchange(part.reshape(tp * groups, 4, own_width)).reshape(tp * groups * 4, own_width)
    mixed_out = pl.pallas_call(
        finish_kernel,
        out_shape=shape((rows, own_width), BF16),
        in_specs=[VMEM] * 2,
        out_specs=VMEM,
        compiler_params=room(4),
        name="finish",
    )(returned, columns)
    return mixed_out, memory_next, norm_next, most.T


def solution(mesh):
    tp = mesh.shape["tp"]
    inner = Mesh(mesh.devices.reshape(mesh.shape["ep"], tp // 2, 2), ("ep", "z", "core"))
    t = ("z", "core")
    every = ("ep", "z", "core")
    in_specs = (
        P("ep", t),
        P(),
        P(),
        P(None, t),
        P(None, t),
        P(None, None, t),
        P(None, None, t),
        P(),
        P(),
        P(),
        P(),
        P("ep", None, t, None),
        P("ep", None, None),
        P("ep", None),
        P(every, None, None),
        P(every, None, None),
        P(every, None, None),
        P("ep", None),
        P("ep", None),
    )
    out_specs = (P("ep", t), P("ep", None, t, None), P("ep", None, None), P("ep", None))
    return jax.shard_map(local, mesh=inner, in_specs=in_specs, out_specs=out_specs, check_vma=False)
```

```python
import functools

import jax
import jax.numpy as jnp
from jax import lax
from jax.experimental import pallas as pl
from jax.experimental.pallas import tpu as pltpu
from jax.sharding import Mesh
from jax.sharding import PartitionSpec as P

EPS = 1e-06
F32 = jnp.float32
BF16 = jnp.bfloat16


def swap_cores(x):
    return lax.ppermute(x, "core", [(0, 1), (1, 0)])


def gather_z(copies):
    own = lax.all_to_all(copies, "z", 0, 0, tiled=True)
    return own, swap_cores(own)


def exchange(x):
    return lax.all_to_all(x, ("z", "core", "ep"), 0, 0, tiled=True)


def hbm(x):
    return pltpu.with_memory_space_constraint(x, pltpu.HBM)


VMEM = pl.BlockSpec(memory_space=pltpu.VMEM)
SMEM = pl.BlockSpec(memory_space=pltpu.SMEM)
HBM = pl.BlockSpec(memory_space=pltpu.HBM)


def room(mib):
    return pltpu.CompilerParams(vmem_limit_bytes=mib * 1024 * 1024)


def shape(dims, dtype=F32):
    return jax.ShapeDtypeStruct(dims, dtype)


def dot(a, b):
    return jnp.dot(a, b, preferred_element_type=F32)


def dot_t(a, b):
    return lax.dot_general(a, b, (((1,), (1,)), ((), ())), preferred_element_type=F32)


def diagonal(n):
    return lax.broadcasted_iota(jnp.int32, (n, n), 0) == lax.broadcasted_iota(jnp.int32, (n, n), 1)


def as_column(row):
    return jnp.sum(jnp.where(diagonal(row.shape[1]), row, 0.0), axis=1, keepdims=True)


def as_row(column):
    return jnp.sum(jnp.where(diagonal(column.shape[0]), column, 0.0), axis=0, keepdims=True)


def low_lanes(rows):
    return lax.broadcasted_iota(jnp.int32, (rows, 128), 1) < 64


def part_copy(source, target, sems, n):
    size = target.shape[0] // sems.shape[0]
    at = pl.ds(pl.multiple_of(n * size, size), size)
    return pltpu.make_async_copy(source.at[at], target.at[at], sems.at[n])


def start(make, count):
    def body(n, carry):
        make(n).start()
        return carry

    lax.fori_loop(0, count, body, 0)


def drain(make, count):
    for n in range(count):
        make(n).wait()


def more_kernel(source, target, sems, *, offset):
    part = functools.partial(part_copy, source.at[pl.ds(offset, target.shape[0])], target, sems)
    start(part, sems.shape[0])
    drain(part, sems.shape[0])


def stage_kernel(mixout, target, sems):
    copies = []
    for m in range(target.shape[0]):
        for h in range(4):
            source = mixout.at[pl.ds(h * 256 + m * 64, 64)]
            copies.append(pltpu.make_async_copy(source, target.at[m, pl.ds(h * 64, 64)], sems.at[m, h]))
    for copy in copies:
        copy.start()
    for copy in copies:
        copy.wait()


def prepare_kernel(
    routes_hbm, weights_hbm, tokens_hbm, wi_hbm, wf_hbm, wq, wk, wv, wo, gain, state, memory,
    wqk, wvo, gain_out, state_out, loaded, wg, columns, picked, base,
    routes, weights, tokens, wi, wf, sems, load_sems,
):
    half = wq.shape[0]
    ends = [
        (routes_hbm, routes),
        (weights_hbm, weights),
        (tokens_hbm, tokens),
        (wi_hbm, wi),
        (wf_hbm, wf),
        (wq, wqk.at[pl.ds(0, half)]),
        (wk, wqk.at[pl.ds(half, half)]),
        (wv, wvo.at[pl.ds(0, half)]),
        (wo, wvo.at[pl.ds(half, half)]),
        (gain, gain_out),
        (state, state_out),
    ]
    copies = [pltpu.make_async_copy(source, target, sems.at[n]) for n, (source, target) in enumerate(ends)]
    for copy in copies:
        copy.start()
    part = functools.partial(part_copy, memory, loaded, load_sems)
    start(part, load_sems.shape[0])
    for copy in copies[:5]:
        copy.wait()
    wg[...] = jnp.concatenate([wi[...].astype(F32), wf[...].astype(F32)], axis=0).astype(BF16)
    count = tokens.shape[0]
    at_row = lax.broadcasted_iota(jnp.int32, (count, count), 0)
    at_column = lax.broadcasted_iota(jnp.int32, (count, count), 1)
    experts = [as_column(routes[k : k + 1, :].astype(F32)) for k in range(2)]
    named = [(expert == at_column.astype(F32)).astype(F32) for expert in experts]
    earlier = (at_column < at_row).astype(F32)
    counts = dot(earlier.astype(BF16), (named[0] + named[1]).astype(BF16))
    total = weights[:1, :] + weights[1:, :]
    lane = lax.broadcasted_iota(jnp.int32, (count, 128), 1)
    out = jnp.zeros((count, 128), F32)
    targets = []
    for k in range(2):
        rank = jnp.sum(counts * named[k], axis=1, keepdims=True)
        target = experts[k] * 4.0 + rank
        out = jnp.where(lane == k, target, out)
        out = jnp.where(lane == 2 + k, as_column(weights[k : k + 1, :] / total), out)
        targets.append(twice(as_row(target)))
    columns[...] = out
    rows = picked.shape[1]
    row = lax.broadcasted_iota(jnp.int32, (rows, 128), 0)
    kind = lax.broadcasted_iota(jnp.int32, (rows, 128), 1) // 64
    r = row % 4
    for n in range(picked.shape[0]):
        first = (row // 4) * 16 + 2 * n
        slot = jnp.where(r == 2, first + kind, -1).astype(F32)
        picked[n] = jnp.where((slot == targets[0]) | (slot == targets[1]), 1.0, 0.0).astype(BF16)
        slot = jnp.where(r < 2, first + r, -1).astype(F32)
        chosen = jnp.where((slot == targets[0]) | (slot == targets[1]), 1.0, 0.0)
        base[n] = dot(chosen[:, :64].astype(BF16), tokens[...]).astype(BF16)
    for copy in copies[5:]:
        copy.wait()
    drain(part, load_sems.shape[0])


def project_kernel(
    first, own, other, gain, wqk, wvo, wg, bias, state, payload, values, gates, most, floor, decay, inflow
):
    even = first[0] == 0
    rows = own.shape[1]
    acc_qk = jnp.zeros((rows, 128), F32)
    acc_vo = jnp.zeros((128, rows), F32)
    acc_g = jnp.zeros((8, rows), F32)
    squares = jnp.zeros((rows, 128), F32)
    for z in range(own.shape[0]):
        a = own[z].astype(F32)
        b = other[z].astype(F32)
        x = jnp.concatenate([jnp.where(even, a, b), jnp.where(even, b, a)], axis=1)
        squares = squares + x[:, :128] * x[:, :128] + x[:, 128:] * x[:, 128:]
        at = pl.ds(z * 256, 256)
        scaled = (x * gain[:, at]).astype(BF16)
        acc_qk = acc_qk + dot_t(scaled, wqk[:, at])
        acc_vo = acc_vo + dot_t(wvo[:, at], scaled)
        acc_g = acc_g + dot_t(wg[:, at], scaled)
    mean = jnp.sum(squares, axis=1, keepdims=True) * (1.0 / (own.shape[0] * 256))
    inverse = lax.rsqrt(mean + EPS)
    inverse_row = as_row(inverse)
    scale = jnp.where(low_lanes(rows), 1.0, 256.0 ** (-0.5))
    out = acc_qk * inverse * scale
    for z in range(own.shape[0]):
        payload[z] = out
    acc_vo = acc_vo * inverse_row
    values[...] = acc_vo[:64]
    gates[...] = jax.nn.sigmoid(acc_vo[64:])
    acc_g = acc_g * inverse_row
    ingate = acc_g[:4]
    forget = acc_g[4:] + bias[...]
    logforget = jnp.minimum(forget, 0.0) - jnp.log1p(jnp.exp(-jnp.abs(forget)))
    carried = logforget + state[...]
    top = jnp.maximum(carried, ingate)
    most[...] = top
    floor[...] = jnp.exp(-top)
    decay[...] = jnp.exp(carried - top)
    inflow[...] = jnp.exp(ingate - top)


def twice(x):
    return jnp.concatenate([x, x], axis=1)


def recall_kernel(
    first, own, other, values, gates, floor, decay, inflow, picked, base, state, more, norm_hbm, memory, message, keys,
    queries, norm, staged, outgoing, late, in_sem, out_sems, sems,
):
    heads = 4
    rows = own.shape[1]
    block = 8
    ready = state.shape[0] + more.shape[0]

    def fetch(i):
        at = pl.ds(i * block, block)
        return pltpu.make_async_copy(memory.at[pl.ds(ready + i * block, block)], late.at[at], sems.at[i])

    start(fetch, late.shape[0] // block)
    norm_copy = pltpu.make_async_copy(norm_hbm, norm, in_sem)
    norm_copy.start()
    even = first[0] == 0
    low = low_lanes(rows)
    for z in range(own.shape[0]):
        a = own[z]
        b = other[z]
        e = jnp.where(even, a, b)
        o = jnp.where(even, b, a)
        at = pl.ds(z * 128, 128)
        queries[:, at] = jnp.where(low, e, pltpu.roll(o, 64, 1))
        staged[:, at] = jnp.where(low, pltpu.roll(e, 64, 1), o)
    key_copy = pltpu.make_async_copy(staged, keys, out_sems.at[0])
    key_copy.start()
    lane = lax.broadcasted_iota(jnp.int32, (16, 128), 1) % 64

    ones = jnp.ones((128, 128), BF16)

    def add(source, offset, i, sums):
        sums = list(sums)
        prods = []
        for j in range(block):
            at = i * block + j
            for h in range(heads):
                prod = source[at, h] * queries[pl.ds(offset + at, 1), pl.ds(h * 256, 256)]
                prods.append(prod[:, :128] + prod[:, 128:])
        prods = jnp.concatenate(prods, axis=0)
        high = prods.astype(BF16)
        totals = dot(high, ones) + dot((prods - high.astype(F32)).astype(BF16), ones)
        for j in range(block):
            here = lane == offset + i * block + j
            for h in range(heads):
                at = (j * heads + h) * 16
                sums[h] = jnp.where(here, totals[at : at + 16], sums[h])
        return tuple(sums)

    def late_step(i, sums):
        fetch(i).wait()
        return add(late, ready, i, sums)

    sums = (jnp.zeros((16, 128), F32),) * heads
    sums = lax.fori_loop(0, state.shape[0] // block, lambda i, sums: add(state, 0, i, sums), sums)
    sums = lax.fori_loop(0, more.shape[0] // block, lambda i, sums: add(more, state.shape[0], i, sums), sums)
    sums = lax.fori_loop(0, late.shape[0] // block, late_step, sums)
    norm_copy.wait()
    half = lax.broadcasted_iota(jnp.int32, (16, 128), 1) < 64
    upper, lower = [], []
    for h in range(heads):
        at = pl.ds(h * 256, 256)
        q = queries[:, at]
        nq = as_row(jnp.sum(norm[:, h, :] * q, axis=1, keepdims=True))
        kq = as_row(jnp.sum(staged[:, at] * q, axis=1, keepdims=True))
        here = pl.ds(h, 1)
        bottom = jnp.abs(decay[here, :] * nq + inflow[here, :] * kq)
        bottom = jnp.maximum(bottom, floor[here, :])
        kept = twice(decay[here, :] / bottom)
        fresh = twice(inflow[here, :] * kq / bottom)
        mine = pl.ds(h * 16, 16)
        gated = twice(gates[mine, :]) * (kept * sums[h] + fresh * twice(values[mine, :]))
        upper.append(jnp.where(half, gated, 0.0))
        lower.append(jnp.where(half, 0.0, gated))
    both = jnp.concatenate(upper + lower, axis=0).astype(BF16)
    sends = []
    for part in range(outgoing.shape[0]):
        out = dot_t(picked[part], both) + base[part].astype(F32)
        outgoing[part] = out.astype(BF16)
        j, c = part // 2, part % 2
        for twin in range(2):
            send = pltpu.make_async_copy(
                outgoing.at[part], message.at[4 * j + 2 * twin + c], out_sems.at[1 + 2 * part + twin]
            )
            send.start()
            sends.append(send)
    for send in sends:
        send.wait()
    key_copy.wait()


def update_kernel(
    decay_scalar, values, decay, inflow, keys_hbm, norm_hbm, memory, memory_next, norm_next,
    keys, norm, norm_out, state, sems, in_sems, out_sems,
):
    heads = 4
    rows = keys.shape[0]
    block = rows // in_sems.shape[0]
    key_copy = pltpu.make_async_copy(keys_hbm, keys, sems.at[0])
    key_copy.start()
    fetch = functools.partial(part_copy, memory, state, in_sems)
    send = functools.partial(part_copy, state, memory_next, out_sems)
    start(fetch, in_sems.shape[0])
    norm_copy = pltpu.make_async_copy(norm_hbm, norm, sems.at[1])
    norm_copy.start()
    key_copy.wait()
    lane = lax.broadcasted_iota(jnp.int32, (16, rows), 1)
    fresh = [values[pl.ds(h * 16, 16), :] * inflow[pl.ds(h, 1), :] for h in range(heads)]

    def step(i, carry):
        fetch(i).wait()
        for j in range(block):
            s = i * block + j
            for h in range(heads):
                column = jnp.sum(jnp.where(lane == s, fresh[h], 0.0), axis=1, keepdims=True)
                key = keys[pl.ds(s, 1), pl.ds(h * 256, 256)]
                state[s, h] = decay_scalar[h, s] * state[s, h] + column * key
        send(i).start()
        return carry

    lax.fori_loop(0, in_sems.shape[0], step, 0)
    norm_copy.wait()
    for h in range(heads):
        here = pl.ds(h, 1)
        kept = as_column(decay[here, :])
        norm_out[:, h, :] = kept * norm[:, h, :] + as_column(inflow[here, :]) * keys[:, pl.ds(h * 256, 256)]
    norm_send = pltpu.make_async_copy(norm_out, norm_next, sems.at[2])
    norm_send.start()
    norm_send.wait()
    drain(send, out_sems.shape[0])


def expert_kernel(
    arrived, gain, staged, mixout, gate_a, gate_b, up_a, up_b, down_a, down_b, out,
    wide, final, weights, downs, sems, weight_sems,
):
    count, groups = arrived.shape[0], arrived.shape[1] // 4

    ready = staged.shape[0]

    def rest(h):
        source = mixout.at[pl.ds(pl.multiple_of(h * 256 + ready * 64, 64), 64)]
        return pltpu.make_async_copy(source, final.at[pl.ds(pl.multiple_of(h * 64, 64), 64)], sems.at[h])

    loads = [
        functools.partial(part_copy, source.at[0], weights.at[n], weight_sems.at[n])
        for n, source in enumerate((gate_a, up_a, gate_b, up_b))
    ]
    loads += [
        functools.partial(part_copy, source.at[0], downs.at[n], weight_sems.at[4 + n])
        for n, source in enumerate((down_a, down_b))
    ]
    for make in [rest] + loads:
        start(make, 4)
    for t in range(count):
        wide[t] = arrived[t].astype(F32)
    low = low_lanes(groups)
    total = jnp.zeros((2 * groups, gain.shape[1]), F32)
    for m in range(count // 4):
        parts, slices = [], []
        for z in range(2):
            t = 4 * m + 2 * z
            e = wide[t, pl.ds(2, groups, stride=4)]
            o = wide[t + 1, pl.ds(2, groups, stride=4)]
            front = jnp.where(low, e, pltpu.roll(o, 64, 1))
            back = jnp.where(low, pltpu.roll(e, 64, 1), o)
            parts.append(jnp.concatenate([front, back], axis=0).astype(BF16))
            slices += [pl.ds(h * 64 + (2 * z + u) * 16, 16) for u in range(2) for h in range(4)]
        if m < ready:
            turned = [staged[m, at, :] for at in slices]
        else:
            drain(rest, 4)
            turned = [final[at, :] for at in slices]
        turned = jnp.concatenate(turned, axis=0)
        total = total + dot(jnp.concatenate(parts, axis=1), turned)
    middle = []
    squares = jnp.zeros((2 * groups, 128), F32)
    for t in range(count):
        rows = [wide[t, pl.ds(b, groups, stride=4)] for b in range(2)]
        piece = jnp.concatenate(rows, axis=0) + total[:, t * 128 : (t + 1) * 128]
        piece = piece.astype(BF16).astype(F32)
        squares = squares + piece * piece
        middle.append(piece)
    mean = jnp.sum(squares, axis=1, keepdims=True) * (1.0 / gain.shape[1])
    inverse = lax.rsqrt(mean + EPS)
    normed = [
        (piece * inverse * gain[:, t * 128 : (t + 1) * 128]).astype(BF16) for t, piece in enumerate(middle)
    ]
    normed = jnp.concatenate(normed, axis=1)
    hidden = []
    for n in range(2):
        drain(loads[2 * n], 4)
        g = dot(normed, weights[2 * n])
        drain(loads[2 * n + 1], 4)
        u = dot(normed, weights[2 * n + 1])
        hidden.append((g * jax.nn.sigmoid(g) * u).astype(BF16))
    part = jnp.zeros((2 * groups, gain.shape[1]), F32)
    for n in range(2):
        drain(loads[4 + n], 4)
        part = part + dot(hidden[n], downs[n])
    for t in range(count):
        piece = part[:, t * 128 : (t + 1) * 128] + 0.5 * middle[t]
        for b in range(2):
            wide[t, pl.ds(b, groups, stride=2)] = piece[b * groups : (b + 1) * groups]
        out[t] = wide[t, : 2 * groups].astype(BF16)


def finish_kernel(returned, columns, out):
    rows, count = columns.shape[0], returned.shape[0]
    q = lax.broadcasted_iota(jnp.int32, (1, count), 1)
    t, g, b = q // 32, (q // 2) % 16, q % 2
    slot = (g * 4 + t // 4) * 4 + 2 * (t % 2) + b
    slot = jnp.broadcast_to(slot.astype(F32), (rows, count))
    total = jnp.zeros((rows, out.shape[1]), F32)
    for k in range(2):
        pick = jnp.where(slot == columns[:, k : k + 1], 1.0, 0.0).astype(BF16)
        total = total + columns[:, 2 + k : 3 + k] * dot(pick, returned[...])
    out[...] = total.astype(BF16)


def local(
    tokens,
    mixer_gain,
    expert_gain,
    query_weight,
    key_weight,
    value_weight,
    outgate_weight,
    ingate_weight,
    forget_weight,
    forget_bias,
    mixout_weight,
    memory_state,
    norm_state,
    max_state,
    expert_gate,
    expert_up,
    expert_down,
    routes,
    route_weights,
):
    rows, own_width = tokens.shape
    width = mixer_gain.shape[0]
    heads, head_dim = norm_state.shape[1:]
    local_values = value_weight.shape[2]
    groups = lax.axis_size("ep")
    tp = lax.axis_size("z") * lax.axis_size("core")
    first = lax.axis_index("core").astype(jnp.int32).reshape(1)
    z = lax.axis_size("z")
    channels = heads * local_values
    features = heads * head_dim

    own, other = gather_z(jnp.broadcast_to(tokens, (z, rows, own_width)))
    turned = [query_weight.T, key_weight.T]
    turned += [jnp.transpose(w, (1, 2, 0)).reshape(channels, width) for w in (value_weight, outgate_weight)]
    turned += [mixer_gain.reshape(1, width), max_state.T, memory_state]
    small = [routes.T, route_weights.T, tokens, ingate_weight.T, forget_weight.T]
    ready, extra = 24, 16
    wqk, wvo, gain, state, loaded, wg, columns, picked, base = pl.pallas_call(
        prepare_kernel,
        out_shape=[
            shape((2 * channels, width), BF16),
            shape((2 * channels, width), BF16),
            shape((1, width)),
            shape((heads, rows)),
            shape((ready, *memory_state.shape[1:])),
            shape((2 * heads, width), BF16),
            shape((rows, 128)),
            shape((tp // 2, groups * 4, 128), BF16),
            shape((tp // 2, groups * 4, own_width), BF16),
        ],
        in_specs=[HBM] * 12,
        out_specs=[VMEM] * 9,
        scratch_shapes=[pltpu.VMEM(x.shape, x.dtype) for x in small]
        + [pltpu.SemaphoreType.DMA((11,)), pltpu.SemaphoreType.DMA((6,))],
        compiler_params=room(6),
        name="prepare",
    )(*(hbm(x) for x in small + turned))
    flat = (channels, rows)
    per_head = (heads, rows)
    payload, values, gates, most, floor, decay, inflow = pl.pallas_call(
        project_kernel,
        out_shape=[shape((z, rows, 128)), shape(flat), shape(flat)] + [shape(per_head)] * 4,
        in_specs=[SMEM] + [VMEM] * 8,
        out_specs=[VMEM] * 7,
        compiler_params=room(4),
        name="project",
    )(first, own, other, gain, wqk, wvo, wg, forget_bias.reshape(heads, 1), state)

    own, other = gather_z(payload)
    more = pl.pallas_call(
        functools.partial(more_kernel, offset=ready),
        out_shape=shape((extra, *memory_state.shape[1:])),
        in_specs=[HBM],
        out_specs=VMEM,
        scratch_shapes=[pltpu.SemaphoreType.DMA((4,))],
        compiler_params=room(4),
        name="more",
    )(hbm(memory_state))
    message, keys = pl.pallas_call(
        recall_kernel,
        out_shape=[pltpu.HBM((tp, groups * 4, own_width), BF16), pltpu.HBM((rows, features), F32)],
        in_specs=[SMEM] + [VMEM] * 11 + [HBM] * 2,
        out_specs=[HBM] * 2,
        scratch_shapes=[
            pltpu.VMEM((rows, features), F32),
            pltpu.VMEM((rows, heads, head_dim), F32),
            pltpu.VMEM((rows, features), F32),
            pltpu.VMEM((tp // 2, groups * 4, own_width), BF16),
            pltpu.VMEM((rows - ready - extra, heads, local_values, head_dim), F32),
            pltpu.SemaphoreType.DMA,
            pltpu.SemaphoreType.DMA((1 + tp,)),
            pltpu.SemaphoreType.DMA(((rows - ready - extra) // 8,)),
        ],
        compiler_params=room(10),
        name="recall",
    )(
        first, own, other, values, gates, floor, decay, inflow, picked, base, loaded, more,
        hbm(norm_state), hbm(memory_state),
    )
    arrived = exchange(message.reshape(tp * groups, 4, own_width)).reshape(tp, groups * 4, own_width)

    memory_next, norm_next = pl.pallas_call(
        update_kernel,
        out_shape=[pltpu.HBM(memory_state.shape, F32), pltpu.HBM(norm_state.shape, F32)],
        in_specs=[SMEM] + [VMEM] * 3 + [HBM] * 3,
        out_specs=[HBM] * 2,
        scratch_shapes=[
            pltpu.VMEM(keys.shape, F32),
            pltpu.VMEM(norm_state.shape, F32),
            pltpu.VMEM(norm_state.shape, F32),
            pltpu.VMEM(memory_state.shape, F32),
            pltpu.SemaphoreType.DMA((3,)),
            pltpu.SemaphoreType.DMA((8,)),
            pltpu.SemaphoreType.DMA((8,)),
        ],
        compiler_params=room(8),
        name="update",
    )(decay, values, decay, inflow, keys, hbm(norm_state), hbm(memory_state))
    staged = pl.pallas_call(
        stage_kernel,
        out_shape=shape((3, features // 4, width), BF16),
        in_specs=[HBM],
        out_specs=VMEM,
        scratch_shapes=[pltpu.SemaphoreType.DMA((3, 4))],
        compiler_params=room(6),
        name="stage",
    )(hbm(mixout_weight))

    twins = [swap_cores(w) for w in (expert_gate, expert_up, expert_down)]
    pairs = [w for mine, twin in zip((expert_gate, expert_up, expert_down), twins) for w in (mine, twin)]
    part = pl.pallas_call(
        expert_kernel,
        out_shape=shape((tp, groups * 2, own_width), BF16),
        in_specs=[VMEM] * 3 + [HBM] * 7,
        out_specs=VMEM,
        scratch_shapes=[
            pltpu.VMEM((tp, groups * 4, own_width), F32),
            pltpu.VMEM((features // 4, width), BF16),
            pltpu.VMEM((4, *expert_gate.shape[1:]), BF16),
            pltpu.VMEM((2, *expert_down.shape[1:]), BF16),
            pltpu.SemaphoreType.DMA((4,)),
            pltpu.SemaphoreType.DMA((6, 4)),
        ],
        compiler_params=room(16),
        name="expert",
    )(arrived, expert_gain.reshape(1, width), staged, hbm(mixout_weight), *(hbm(w) for w in pairs))
    returned = exchange(part.reshape(tp * groups, 2, own_width)).reshape(tp * groups * 2, own_width)
    mixed_out = pl.pallas_call(
        finish_kernel,
        out_shape=shape((rows, own_width), BF16),
        in_specs=[VMEM] * 2,
        out_specs=VMEM,
        compiler_params=room(4),
        name="finish",
    )(returned, columns)
    return mixed_out, memory_next, norm_next, most.T


def solution(mesh):
    tp = mesh.shape["tp"]
    inner = Mesh(mesh.devices.reshape(mesh.shape["ep"], tp // 2, 2), ("ep", "z", "core"))
    t = ("z", "core")
    every = ("ep", "z", "core")
    in_specs = (
        P("ep", t),
        P(),
        P(),
        P(None, t),
        P(None, t),
        P(None, None, t),
        P(None, None, t),
        P(),
        P(),
        P(),
        P(),
        P("ep", None, t, None),
        P("ep", None, None),
        P("ep", None),
        P(every, None, None),
        P(every, None, None),
        P(every, None, None),
        P("ep", None),
        P("ep", None),
    )
    out_specs = (P("ep", t), P("ep", None, t, None), P("ep", None, None), P("ep", None))
    return jax.shard_map(local, mesh=inner, in_specs=in_specs, out_specs=out_specs, check_vma=False)
```

```python
import functools

import jax
import jax.numpy as jnp
from jax import lax
from jax.experimental import pallas as pl
from jax.experimental.pallas import tpu as pltpu
from jax.sharding import Mesh
from jax.sharding import PartitionSpec as P

EPS = 1e-06
F32 = jnp.float32
BF16 = jnp.bfloat16


def swap_cores(x):
    return lax.ppermute(x, "core", [(0, 1), (1, 0)])


def gather_z(copies):
    own = lax.all_to_all(copies, "z", 0, 0, tiled=True)
    return own, swap_cores(own)


def exchange(x):
    return lax.all_to_all(x, ("z", "core", "ep"), 0, 0, tiled=True)


def hbm(x):
    return pltpu.with_memory_space_constraint(x, pltpu.HBM)


VMEM = pl.BlockSpec(memory_space=pltpu.VMEM)
SMEM = pl.BlockSpec(memory_space=pltpu.SMEM)
HBM = pl.BlockSpec(memory_space=pltpu.HBM)


def room(mib):
    return pltpu.CompilerParams(vmem_limit_bytes=mib * 1024 * 1024)


def shape(dims, dtype=F32):
    return jax.ShapeDtypeStruct(dims, dtype)


def dot(a, b):
    return jnp.dot(a, b, preferred_element_type=F32)


def dot_t(a, b):
    return lax.dot_general(a, b, (((1,), (1,)), ((), ())), preferred_element_type=F32)


def diagonal(n):
    return lax.broadcasted_iota(jnp.int32, (n, n), 0) == lax.broadcasted_iota(jnp.int32, (n, n), 1)


def as_column(row):
    return jnp.sum(jnp.where(diagonal(row.shape[1]), row, 0.0), axis=1, keepdims=True)


def as_row(column):
    return jnp.sum(jnp.where(diagonal(column.shape[0]), column, 0.0), axis=0, keepdims=True)


def low_lanes(rows):
    return lax.broadcasted_iota(jnp.int32, (rows, 128), 1) < 64


def part_copy(source, target, sems, n):
    size = target.shape[0] // sems.shape[0]
    at = pl.ds(pl.multiple_of(n * size, size), size)
    return pltpu.make_async_copy(source.at[at], target.at[at], sems.at[n])


def start(make, count):
    def body(n, carry):
        make(n).start()
        return carry

    lax.fori_loop(0, count, body, 0)


def drain(make, count):
    for n in range(count):
        make(n).wait()


def more_kernel(source, target, sems, *, offset):
    part = functools.partial(part_copy, source.at[pl.ds(offset, target.shape[0])], target, sems)
    start(part, sems.shape[0])
    drain(part, sems.shape[0])


def stage_kernel(mixout, target, sems):
    copies = []
    for m in range(target.shape[0]):
        for h in range(4):
            source = mixout.at[pl.ds(h * 256 + m * 64, 64)]
            copies.append(pltpu.make_async_copy(source, target.at[m, pl.ds(h * 64, 64)], sems.at[m, h]))
    for copy in copies:
        copy.start()
    for copy in copies:
        copy.wait()


def prepare_kernel(
    place, routes_hbm, weights_hbm, tokens_hbm, wi_hbm, wf_hbm, norm_hbm, wq, wk, wv, wo, gain, state, memory,
    wqk, wvo, gain_out, state_out, loaded, wg, columns, picked, base, norm_own,
    routes, weights, tokens, wi, wf, norm, sems, load_sems,
):
    half = wq.shape[0]
    ends = [
        (routes_hbm, routes),
        (weights_hbm, weights),
        (tokens_hbm, tokens),
        (wi_hbm, wi),
        (wf_hbm, wf),
        (norm_hbm, norm),
        (wq, wqk.at[pl.ds(0, half)]),
        (wk, wqk.at[pl.ds(half, half)]),
        (wv, wvo.at[pl.ds(0, half)]),
        (wo, wvo.at[pl.ds(half, half)]),
        (gain, gain_out),
        (state, state_out),
    ]
    copies = [pltpu.make_async_copy(source, target, sems.at[n]) for n, (source, target) in enumerate(ends)]
    for copy in copies:
        copy.start()
    part = functools.partial(part_copy, memory, loaded, load_sems)
    start(part, load_sems.shape[0])
    for copy in copies[:6]:
        copy.wait()
    mine = jnp.zeros(norm_own.shape, F32)
    for z in range(8):
        mine = jnp.where(place[1] == z, norm[:, z // 2, pl.ds((z % 2) * 128, 128)], mine)
    norm_own[...] = jnp.where(place[0] == 0, mine, pltpu.roll(mine, 64, 1))
    wg[...] = jnp.concatenate([wi[...].astype(F32), wf[...].astype(F32)], axis=0).astype(BF16)
    count = tokens.shape[0]
    at_row = lax.broadcasted_iota(jnp.int32, (count, count), 0)
    at_column = lax.broadcasted_iota(jnp.int32, (count, count), 1)
    experts = [as_column(routes[k : k + 1, :].astype(F32)) for k in range(2)]
    named = [(expert == at_column.astype(F32)).astype(F32) for expert in experts]
    earlier = (at_column < at_row).astype(F32)
    counts = dot(earlier.astype(BF16), (named[0] + named[1]).astype(BF16))
    total = weights[:1, :] + weights[1:, :]
    lane = lax.broadcasted_iota(jnp.int32, (count, 128), 1)
    out = jnp.zeros((count, 128), F32)
    targets = []
    for k in range(2):
        rank = jnp.sum(counts * named[k], axis=1, keepdims=True)
        target = experts[k] * 4.0 + rank
        out = jnp.where(lane == k, target, out)
        out = jnp.where(lane == 2 + k, as_column(weights[k : k + 1, :] / total), out)
        targets.append(twice(as_row(target)))
    columns[...] = out
    rows = picked.shape[1]
    row = lax.broadcasted_iota(jnp.int32, (rows, 128), 0)
    kind = lax.broadcasted_iota(jnp.int32, (rows, 128), 1) // 64
    r = row % 4
    for n in range(picked.shape[0]):
        first = (row // 4) * 16 + 2 * n
        slot = jnp.where(r == 2, first + kind, -1).astype(F32)
        picked[n] = jnp.where((slot == targets[0]) | (slot == targets[1]), 1.0, 0.0).astype(BF16)
        slot = jnp.where(r < 2, first + r, -1).astype(F32)
        chosen = jnp.where((slot == targets[0]) | (slot == targets[1]), 1.0, 0.0)
        base[n] = dot(chosen[:, :64].astype(BF16), tokens[...]).astype(BF16)
    for copy in copies[6:]:
        copy.wait()
    drain(part, load_sems.shape[0])


def project_kernel(
    first, own, other, gain, wqk, wvo, wg, bias, state, norm, payload, values, gates, most, floor, decay, inflow
):
    even = first[0] == 0
    rows = own.shape[1]
    acc_qk = jnp.zeros((rows, 128), F32)
    acc_vo = jnp.zeros((128, rows), F32)
    acc_g = jnp.zeros((8, rows), F32)
    squares = jnp.zeros((rows, 128), F32)
    for z in range(own.shape[0]):
        a = own[z].astype(F32)
        b = other[z].astype(F32)
        x = jnp.concatenate([jnp.where(even, a, b), jnp.where(even, b, a)], axis=1)
        squares = squares + x[:, :128] * x[:, :128] + x[:, 128:] * x[:, 128:]
        at = pl.ds(z * 256, 256)
        scaled = (x * gain[:, at]).astype(BF16)
        acc_qk = acc_qk + dot_t(scaled, wqk[:, at])
        acc_vo = acc_vo + dot_t(wvo[:, at], scaled)
        acc_g = acc_g + dot_t(wg[:, at], scaled)
    mean = jnp.sum(squares, axis=1, keepdims=True) * (1.0 / (own.shape[0] * 256))
    inverse = lax.rsqrt(mean + EPS)
    inverse_row = as_row(inverse)
    scale = jnp.where(low_lanes(rows), 1.0, 256.0 ** (-0.5))
    out = acc_qk * inverse * scale
    low = low_lanes(rows)
    extra = []
    for product in (out * norm[...], out * pltpu.roll(out, 64, 1)):
        left = twice(as_row(jnp.sum(jnp.where(low, product, 0.0), axis=1, keepdims=True)))
        for _ in range(3):
            extra.append(left.astype(BF16).astype(F32))
            left = left - extra[-1]
    index = lax.broadcasted_iota(jnp.int32, (16, 128), 0)
    tail = jnp.zeros((16, 128), F32)
    for n, term in enumerate(extra):
        tail = jnp.where(index == n, term, tail)
    out = jnp.concatenate([out, tail], axis=0).astype(BF16)
    for z in range(own.shape[0]):
        payload[z] = out
    acc_vo = acc_vo * inverse_row
    values[...] = acc_vo[:64]
    gates[...] = jax.nn.sigmoid(acc_vo[64:])
    acc_g = acc_g * inverse_row
    ingate = acc_g[:4]
    forget = acc_g[4:] + bias[...]
    logforget = jnp.minimum(forget, 0.0) - jnp.log1p(jnp.exp(-jnp.abs(forget)))
    carried = logforget + state[...]
    top = jnp.maximum(carried, ingate)
    most[...] = top
    floor[...] = jnp.exp(-top)
    decay[...] = jnp.exp(carried - top)
    inflow[...] = jnp.exp(ingate - top)


def twice(x):
    return jnp.concatenate([x, x], axis=1)


def recall_kernel(
    first, own, other, values, gates, floor, decay, inflow, picked, base, state, more, memory, message, keys,
    queries, staged, outgoing, late, out_sems, sems,
):
    heads = 4
    rows = staged.shape[0]
    block = 8
    ready = state.shape[0] + more.shape[0]

    def fetch(i):
        at = pl.ds(i * block, block)
        return pltpu.make_async_copy(memory.at[pl.ds(ready + i * block, block)], late.at[at], sems.at[i])

    start(fetch, late.shape[0] // block)
    even = first[0] == 0
    low = low_lanes(rows)
    for z in range(own.shape[0]):
        a = own[z, :rows].astype(F32)
        b = other[z, :rows].astype(F32)
        e = jnp.where(even, a, b)
        o = jnp.where(even, b, a)
        at = pl.ds(z * 128, 128)
        queries[:, at] = jnp.where(low, e, pltpu.roll(o, 64, 1))
        staged[:, at] = jnp.where(low, pltpu.roll(e, 64, 1), o)
    key_copy = pltpu.make_async_copy(staged, keys, out_sems.at[0])
    key_copy.start()
    lane = lax.broadcasted_iota(jnp.int32, (16, 128), 1) % 64

    ones = jnp.ones((128, 128), BF16)

    def add(source, offset, i, sums):
        block = 4
        sums = list(sums)
        prods = []
        for j in range(block):
            at = i * block + j
            for h in range(heads):
                prod = source[at, h] * queries[pl.ds(offset + at, 1), pl.ds(h * 256, 256)]
                prods.append(prod[:, :128] + prod[:, 128:])
        prods = jnp.concatenate(prods, axis=0)
        high = prods.astype(BF16)
        totals = dot(high, ones) + dot((prods - high.astype(F32)).astype(BF16), ones)
        for j in range(block):
            here = lane == offset + i * block + j
            for h in range(heads):
                at = (j * heads + h) * 16
                sums[h] = jnp.where(here, totals[at : at + 16], sums[h])
        return tuple(sums)

    sums = (jnp.zeros((16, 128), F32),) * heads
    for i in range(state.shape[0] // 4):
        sums = add(state, 0, i, sums)
    for i in range(more.shape[0] // 4):
        sums = add(more, state.shape[0], i, sums)
    kept, fresh = [], []
    for h in range(heads):
        tail = sum(shard[z, rows:].astype(F32) for shard in (own, other) for z in (2 * h, 2 * h + 1))
        nq = tail[0:1] + tail[1:2] + tail[2:3]
        kq = tail[3:4] + tail[4:5] + tail[5:6]
        here = pl.ds(h, 1)
        down, up = twice(decay[here, :]), twice(inflow[here, :])
        bottom = jnp.maximum(jnp.abs(down * nq + up * kq), twice(floor[here, :]))
        kept.append(down / bottom)
        fresh.append(up * kq / bottom)
    for i in range(late.shape[0] // block):
        fetch(i).wait()
        for j in range(block // 4):
            sums = add(late, ready, i * (block // 4) + j, sums)
    half = lax.broadcasted_iota(jnp.int32, (16, 128), 1) < 64
    upper, lower = [], []
    for h in range(heads):
        mine = pl.ds(h * 16, 16)
        gated = twice(gates[mine, :]) * (kept[h] * sums[h] + fresh[h] * twice(values[mine, :]))
        upper.append(jnp.where(half, gated, 0.0))
        lower.append(jnp.where(half, 0.0, gated))
    both = jnp.concatenate(upper + lower, axis=0).astype(BF16)
    sends = []
    for part in range(outgoing.shape[0]):
        out = dot_t(picked[part], both) + base[part].astype(F32)
        outgoing[part] = out.astype(BF16)
        j, c = part // 2, part % 2
        for twin in range(2):
            send = pltpu.make_async_copy(
                outgoing.at[part], message.at[4 * j + 2 * twin + c], out_sems.at[1 + 2 * part + twin]
            )
            send.start()
            sends.append(send)
    for send in sends:
        send.wait()
    key_copy.wait()


def update_kernel(
    decay_scalar, values, decay, inflow, most, keys_hbm, norm_hbm, memory, memory_next, norm_next, most_next,
    keys, norm, norm_out, state, sems, in_sems, out_sems,
):
    heads = 4
    rows = keys.shape[0]
    block = rows // in_sems.shape[0]
    key_copy = pltpu.make_async_copy(keys_hbm, keys, sems.at[0])
    key_copy.start()
    most_copy = pltpu.make_async_copy(most, most_next, sems.at[3])
    most_copy.start()
    fetch = functools.partial(part_copy, memory, state, in_sems)
    send = functools.partial(part_copy, state, memory_next, out_sems)
    start(fetch, in_sems.shape[0])
    norm_copy = pltpu.make_async_copy(norm_hbm, norm, sems.at[1])
    norm_copy.start()
    key_copy.wait()
    lane = lax.broadcasted_iota(jnp.int32, (16, rows), 1)
    fresh = [values[pl.ds(h * 16, 16), :] * inflow[pl.ds(h, 1), :] for h in range(heads)]

    def step(i, carry):
        fetch(i).wait()
        for j in range(block):
            s = i * block + j
            for h in range(heads):
                column = jnp.sum(jnp.where(lane == s, fresh[h], 0.0), axis=1, keepdims=True)
                key = keys[pl.ds(s, 1), pl.ds(h * 256, 256)]
                state[s, h] = decay_scalar[h, s] * state[s, h] + column * key
        send(i).start()
        return carry

    lax.fori_loop(0, in_sems.shape[0], step, 0)
    norm_copy.wait()
    for h in range(heads):
        here = pl.ds(h, 1)
        kept = as_column(decay[here, :])
        norm_out[:, h, :] = kept * norm[:, h, :] + as_column(inflow[here, :]) * keys[:, pl.ds(h * 256, 256)]
    norm_send = pltpu.make_async_copy(norm_out, norm_next, sems.at[2])
    norm_send.start()
    norm_send.wait()
    most_copy.wait()
    drain(send, out_sems.shape[0])


def expert_kernel(
    arrived, gain, staged, mixout, gate_a, gate_b, up_a, up_b, down_a, down_b, out,
    wide, final, weights, downs, sems, weight_sems,
):
    count, groups = arrived.shape[0], arrived.shape[1] // 4

    ready = staged.shape[0]

    def rest(h):
        source = mixout.at[pl.ds(pl.multiple_of(h * 256 + ready * 64, 64), 64)]
        return pltpu.make_async_copy(source, final.at[pl.ds(pl.multiple_of(h * 64, 64), 64)], sems.at[h])

    loads = [
        functools.partial(part_copy, source.at[0], weights.at[n], weight_sems.at[n])
        for n, source in enumerate((gate_a, up_a, gate_b, up_b))
    ]
    loads += [
        functools.partial(part_copy, source.at[0], downs.at[n], weight_sems.at[4 + n])
        for n, source in enumerate((down_a, down_b))
    ]
    for make in [rest] + loads:
        start(make, 4)
    for t in range(count):
        wide[t] = arrived[t].astype(F32)
    low = low_lanes(groups)
    total = jnp.zeros((2 * groups, gain.shape[1]), F32)
    for m in range(count // 4):
        parts, slices = [], []
        for z in range(2):
            t = 4 * m + 2 * z
            e = wide[t, pl.ds(2, groups, stride=4)]
            o = wide[t + 1, pl.ds(2, groups, stride=4)]
            front = jnp.where(low, e, pltpu.roll(o, 64, 1))
            back = jnp.where(low, pltpu.roll(e, 64, 1), o)
            parts.append(jnp.concatenate([front, back], axis=0).astype(BF16))
            slices += [pl.ds(h * 64 + (2 * z + u) * 16, 16) for u in range(2) for h in range(4)]
        if m < ready:
            turned = [staged[m, at, :] for at in slices]
        else:
            drain(rest, 4)
            turned = [final[at, :] for at in slices]
        turned = jnp.concatenate(turned, axis=0)
        total = total + dot(jnp.concatenate(parts, axis=1), turned)
    middle = []
    squares = jnp.zeros((2 * groups, 128), F32)
    for t in range(count):
        rows = [wide[t, pl.ds(b, groups, stride=4)] for b in range(2)]
        piece = jnp.concatenate(rows, axis=0) + total[:, t * 128 : (t + 1) * 128]
        piece = piece.astype(BF16).astype(F32)
        squares = squares + piece * piece
        middle.append(piece)
    mean = jnp.sum(squares, axis=1, keepdims=True) * (1.0 / gain.shape[1])
    inverse = lax.rsqrt(mean + EPS)
    normed = [
        (piece * inverse * gain[:, t * 128 : (t + 1) * 128]).astype(BF16) for t, piece in enumerate(middle)
    ]
    normed = jnp.concatenate(normed, axis=1)
    hidden = []
    for n in range(2):
        drain(loads[2 * n], 4)
        g = dot(normed, weights[2 * n])
        drain(loads[2 * n + 1], 4)
        u = dot(normed, weights[2 * n + 1])
        hidden.append((g * jax.nn.sigmoid(g) * u).astype(BF16))
    part = jnp.zeros((2 * groups, gain.shape[1]), F32)
    for n in range(2):
        drain(loads[4 + n], 4)
        part = part + dot(hidden[n], downs[n])
    for t in range(count):
        piece = part[:, t * 128 : (t + 1) * 128] + 0.5 * middle[t]
        for b in range(2):
            wide[t, pl.ds(b, groups, stride=2)] = piece[b * groups : (b + 1) * groups]
        out[t] = wide[t, : 2 * groups].astype(BF16)


def finish_kernel(returned, columns, out):
    rows, count = columns.shape[0], returned.shape[0]
    q = lax.broadcasted_iota(jnp.int32, (1, count), 1)
    t, g, b = q // 32, (q // 2) % 16, q % 2
    slot = (g * 4 + t // 4) * 4 + 2 * (t % 2) + b
    slot = jnp.broadcast_to(slot.astype(F32), (rows, count))
    total = jnp.zeros((rows, out.shape[1]), F32)
    for k in range(2):
        pick = jnp.where(slot == columns[:, k : k + 1], 1.0, 0.0).astype(BF16)
        total = total + columns[:, 2 + k : 3 + k] * dot(pick, returned[...])
    out[...] = total.astype(BF16)


def local(
    tokens,
    mixer_gain,
    expert_gain,
    query_weight,
    key_weight,
    value_weight,
    outgate_weight,
    ingate_weight,
    forget_weight,
    forget_bias,
    mixout_weight,
    memory_state,
    norm_state,
    max_state,
    expert_gate,
    expert_up,
    expert_down,
    routes,
    route_weights,
):
    rows, own_width = tokens.shape
    width = mixer_gain.shape[0]
    heads, head_dim = norm_state.shape[1:]
    local_values = value_weight.shape[2]
    groups = lax.axis_size("ep")
    tp = lax.axis_size("z") * lax.axis_size("core")
    place = jnp.stack([lax.axis_index("core"), lax.axis_index("z")]).astype(jnp.int32)
    z = lax.axis_size("z")
    channels = heads * local_values
    features = heads * head_dim

    own, other = gather_z(jnp.broadcast_to(tokens, (z, rows, own_width)))
    turned = [query_weight.T, key_weight.T]
    turned += [jnp.transpose(w, (1, 2, 0)).reshape(channels, width) for w in (value_weight, outgate_weight)]
    turned += [mixer_gain.reshape(1, width), max_state.T, memory_state]
    small = [routes.T, route_weights.T, tokens, ingate_weight.T, forget_weight.T, norm_state]
    ready, extra = 24, 16
    wqk, wvo, gain, state, loaded, wg, columns, picked, base, norm_own = pl.pallas_call(
        prepare_kernel,
        out_shape=[
            shape((2 * channels, width), BF16),
            shape((2 * channels, width), BF16),
            shape((1, width)),
            shape((heads, rows)),
            shape((ready, *memory_state.shape[1:])),
            shape((2 * heads, width), BF16),
            shape((rows, 128)),
            shape((tp // 2, groups * 4, 128), BF16),
            shape((tp // 2, groups * 4, own_width), BF16),
            shape((rows, 128)),
        ],
        in_specs=[SMEM] + [HBM] * 13,
        out_specs=[VMEM] * 10,
        scratch_shapes=[pltpu.VMEM(x.shape, x.dtype) for x in small]
        + [pltpu.SemaphoreType.DMA((12,)), pltpu.SemaphoreType.DMA((6,))],
        compiler_params=room(6),
        name="prepare",
    )(place, *(hbm(x) for x in small + turned))
    flat = (channels, rows)
    per_head = (heads, rows)
    payload, values, gates, most, floor, decay, inflow = pl.pallas_call(
        project_kernel,
        out_shape=[shape((z, rows + 16, 128), BF16), shape(flat), shape(flat)] + [shape(per_head)] * 4,
        in_specs=[SMEM] + [VMEM] * 9,
        out_specs=[VMEM] * 7,
        compiler_params=room(4),
        name="project",
    )(place, own, other, gain, wqk, wvo, wg, forget_bias.reshape(heads, 1), state, norm_own)

    own, other = gather_z(payload)
    more = pl.pallas_call(
        functools.partial(more_kernel, offset=ready),
        out_shape=shape((extra, *memory_state.shape[1:])),
        in_specs=[HBM],
        out_specs=VMEM,
        scratch_shapes=[pltpu.SemaphoreType.DMA((4,))],
        compiler_params=room(4),
        name="more",
    )(hbm(memory_state))
    message, keys = pl.pallas_call(
        recall_kernel,
        out_shape=[pltpu.HBM((tp, groups * 4, own_width), BF16), pltpu.HBM((rows, features), F32)],
        in_specs=[SMEM] + [VMEM] * 11 + [HBM],
        out_specs=[HBM] * 2,
        scratch_shapes=[
            pltpu.VMEM((rows, features), F32),
            pltpu.VMEM((rows, features), F32),
            pltpu.VMEM((tp // 2, groups * 4, own_width), BF16),
            pltpu.VMEM((rows - ready - extra, heads, local_values, head_dim), F32),
            pltpu.SemaphoreType.DMA((1 + tp,)),
            pltpu.SemaphoreType.DMA(((rows - ready - extra) // 8,)),
        ],
        compiler_params=room(10),
        name="recall",
    )(
        place, own, other, values, gates, floor, decay, inflow, picked, base, loaded, more,
        hbm(memory_state),
    )
    arrived = exchange(message.reshape(tp * groups, 4, own_width)).reshape(tp, groups * 4, own_width)

    memory_next, norm_next, most = pl.pallas_call(
        update_kernel,
        out_shape=[pltpu.HBM(x.shape, F32) for x in (memory_state, norm_state, most)],
        in_specs=[SMEM] + [VMEM] * 4 + [HBM] * 3,
        out_specs=[HBM] * 3,
        scratch_shapes=[
            pltpu.VMEM(keys.shape, F32),
            pltpu.VMEM(norm_state.shape, F32),
            pltpu.VMEM(norm_state.shape, F32),
            pltpu.VMEM(memory_state.shape, F32),
            pltpu.SemaphoreType.DMA((4,)),
            pltpu.SemaphoreType.DMA((8,)),
            pltpu.SemaphoreType.DMA((8,)),
        ],
        compiler_params=room(8),
        name="update",
    )(decay, values, decay, inflow, most, keys, hbm(norm_state), hbm(memory_state))
    staged = pl.pallas_call(
        stage_kernel,
        out_shape=shape((3, features // 4, width), BF16),
        in_specs=[HBM],
        out_specs=VMEM,
        scratch_shapes=[pltpu.SemaphoreType.DMA((3, 4))],
        compiler_params=room(6),
        name="stage",
    )(hbm(mixout_weight))

    twins = [swap_cores(w) for w in (expert_gate, expert_up, expert_down)]
    pairs = [w for mine, twin in zip((expert_gate, expert_up, expert_down), twins) for w in (mine, twin)]
    part = pl.pallas_call(
        expert_kernel,
        out_shape=shape((tp, groups * 2, own_width), BF16),
        in_specs=[VMEM] * 3 + [HBM] * 7,
        out_specs=VMEM,
        scratch_shapes=[
            pltpu.VMEM((tp, groups * 4, own_width), F32),
            pltpu.VMEM((features // 4, width), BF16),
            pltpu.VMEM((4, *expert_gate.shape[1:]), BF16),
            pltpu.VMEM((2, *expert_down.shape[1:]), BF16),
            pltpu.SemaphoreType.DMA((4,)),
            pltpu.SemaphoreType.DMA((6, 4)),
        ],
        compiler_params=room(16),
        name="expert",
    )(arrived, expert_gain.reshape(1, width), staged, hbm(mixout_weight), *(hbm(w) for w in pairs))
    returned = exchange(part.reshape(tp * groups, 2, own_width)).reshape(tp * groups * 2, own_width)
    mixed_out = pl.pallas_call(
        finish_kernel,
        out_shape=shape((rows, own_width), BF16),
        in_specs=[VMEM] * 2,
        out_specs=VMEM,
        compiler_params=room(4),
        name="finish",
    )(returned, columns)
    return mixed_out, memory_next, norm_next, most.T


def solution(mesh):
    tp = mesh.shape["tp"]
    inner = Mesh(mesh.devices.reshape(mesh.shape["ep"], tp // 2, 2), ("ep", "z", "core"))
    t = ("z", "core")
    every = ("ep", "z", "core")
    in_specs = (
        P("ep", t),
        P(),
        P(),
        P(None, t),
        P(None, t),
        P(None, None, t),
        P(None, None, t),
        P(),
        P(),
        P(),
        P(),
        P("ep", None, t, None),
        P("ep", None, None),
        P("ep", None),
        P(every, None, None),
        P(every, None, None),
        P(every, None, None),
        P("ep", None),
        P("ep", None),
    )
    out_specs = (P("ep", t), P("ep", None, t, None), P("ep", None, None), P("ep", None))
    return jax.shard_map(local, mesh=inner, in_specs=in_specs, out_specs=out_specs, check_vma=False)
```

```python
import functools

import jax
import jax.numpy as jnp
from jax import lax
from jax.experimental import pallas as pl
from jax.experimental.pallas import tpu as pltpu
from jax.sharding import Mesh
from jax.sharding import PartitionSpec as P

EPS = 1e-06
F32 = jnp.float32
BF16 = jnp.bfloat16


def swap_cores(x):
    return lax.ppermute(x, "core", [(0, 1), (1, 0)])


def gather_z(copies):
    own = lax.all_to_all(copies, "z", 0, 0, tiled=True)
    return own, swap_cores(own)


def exchange(x):
    return lax.all_to_all(x, ("z", "core", "ep"), 0, 0, tiled=True)


def hbm(x):
    return pltpu.with_memory_space_constraint(x, pltpu.HBM)


VMEM = pl.BlockSpec(memory_space=pltpu.VMEM)
SMEM = pl.BlockSpec(memory_space=pltpu.SMEM)
HBM = pl.BlockSpec(memory_space=pltpu.HBM)


def room(mib):
    return pltpu.CompilerParams(vmem_limit_bytes=mib * 1024 * 1024)


def shape(dims, dtype=F32):
    return jax.ShapeDtypeStruct(dims, dtype)


def dot(a, b):
    return jnp.dot(a, b, preferred_element_type=F32)


def dot_t(a, b):
    return lax.dot_general(a, b, (((1,), (1,)), ((), ())), preferred_element_type=F32)


def diagonal(n):
    return lax.broadcasted_iota(jnp.int32, (n, n), 0) == lax.broadcasted_iota(jnp.int32, (n, n), 1)


def as_column(row):
    return jnp.sum(jnp.where(diagonal(row.shape[1]), row, 0.0), axis=1, keepdims=True)


def as_row(column):
    return jnp.sum(jnp.where(diagonal(column.shape[0]), column, 0.0), axis=0, keepdims=True)


def low_lanes(rows):
    return lax.broadcasted_iota(jnp.int32, (rows, 128), 1) < 64


def part_copy(source, target, sems, n):
    size = target.shape[0] // sems.shape[0]
    at = pl.ds(pl.multiple_of(n * size, size), size)
    return pltpu.make_async_copy(source.at[at], target.at[at], sems.at[n])


def start(make, count):
    def body(n, carry):
        make(n).start()
        return carry

    lax.fori_loop(0, count, body, 0)


def drain(make, count):
    for n in range(count):
        make(n).wait()


def more_kernel(source, target, sems, *, offset):
    part = functools.partial(part_copy, source.at[pl.ds(offset, target.shape[0])], target, sems)
    start(part, sems.shape[0])
    drain(part, sems.shape[0])


def stage_kernel(mixout, target, sems):
    copies = []
    for m in range(target.shape[0]):
        for h in range(4):
            source = mixout.at[pl.ds(h * 256 + m * 64, 64)]
            copies.append(pltpu.make_async_copy(source, target.at[m, pl.ds(h * 64, 64)], sems.at[m, h]))
    for copy in copies:
        copy.start()
    for copy in copies:
        copy.wait()


def prepare_kernel(
    place, routes_hbm, weights_hbm, tokens_hbm, wi_hbm, wf_hbm, norm_hbm, wq, wk, wv, wo, gain, state, memory,
    wqk, wvo, gain_out, state_out, loaded, wg, columns, picked, base, norm_own,
    routes, weights, tokens, wi, wf, norm, sems, load_sems,
):
    half = wq.shape[0]
    ends = [
        (routes_hbm, routes),
        (weights_hbm, weights),
        (tokens_hbm, tokens),
        (wi_hbm, wi),
        (wf_hbm, wf),
        (norm_hbm, norm),
        (wq, wqk.at[pl.ds(0, half)]),
        (wk, wqk.at[pl.ds(half, half)]),
        (wv, wvo.at[pl.ds(0, half)]),
        (wo, wvo.at[pl.ds(half, half)]),
        (gain, gain_out),
        (state, state_out),
    ]
    copies = [pltpu.make_async_copy(source, target, sems.at[n]) for n, (source, target) in enumerate(ends)]
    for copy in copies:
        copy.start()
    part = functools.partial(part_copy, memory, loaded, load_sems)
    start(part, load_sems.shape[0])
    for copy in copies[:6]:
        copy.wait()
    mine = jnp.zeros(norm_own.shape, F32)
    for z in range(8):
        mine = jnp.where(place[1:2, :] == z, norm[:, z // 2, pl.ds((z % 2) * 128, 128)], mine)
    norm_own[...] = jnp.where(place[:1, :] == 0, mine, pltpu.roll(mine, 64, 1))
    wg[...] = jnp.concatenate([wi[...].astype(F32), wf[...].astype(F32)], axis=0).astype(BF16)
    count = tokens.shape[0]
    at_row = lax.broadcasted_iota(jnp.int32, (count, count), 0)
    at_column = lax.broadcasted_iota(jnp.int32, (count, count), 1)
    experts = [as_column(routes[k : k + 1, :].astype(F32)) for k in range(2)]
    named = [(expert == at_column.astype(F32)).astype(F32) for expert in experts]
    earlier = (at_column < at_row).astype(F32)
    counts = dot(earlier.astype(BF16), (named[0] + named[1]).astype(BF16))
    total = weights[:1, :] + weights[1:, :]
    lane = lax.broadcasted_iota(jnp.int32, (count, 128), 1)
    out = jnp.zeros((count, 128), F32)
    targets = []
    for k in range(2):
        rank = jnp.sum(counts * named[k], axis=1, keepdims=True)
        target = experts[k] * 4.0 + rank
        out = jnp.where(lane == k, target, out)
        out = jnp.where(lane == 2 + k, as_column(weights[k : k + 1, :] / total), out)
        targets.append(twice(as_row(target)))
    columns[...] = out
    rows = picked.shape[1]
    row = lax.broadcasted_iota(jnp.int32, (rows, 128), 0)
    kind = lax.broadcasted_iota(jnp.int32, (rows, 128), 1) // 64
    r = row % 4
    for n in range(picked.shape[0]):
        first = (row // 4) * 16 + 2 * n
        slot = jnp.where(r == 2, first + kind, -1).astype(F32)
        picked[n] = jnp.where((slot == targets[0]) | (slot == targets[1]), 1.0, 0.0).astype(BF16)
        slot = jnp.where(r < 2, first + r, -1).astype(F32)
        chosen = jnp.where((slot == targets[0]) | (slot == targets[1]), 1.0, 0.0)
        base[n] = dot(chosen[:, :64].astype(BF16), tokens[...]).astype(BF16)
    for copy in copies[6:]:
        copy.wait()
    drain(part, load_sems.shape[0])


def project_kernel(
    first, own, other, gain, wqk, wvo, wg, bias, state, norm, payload, values, gates, most, floor, decay, inflow
):
    even = first[:1, :] == 0
    rows = own.shape[1]
    acc_qk = jnp.zeros((rows, 128), F32)
    acc_vo = jnp.zeros((128, rows), F32)
    acc_g = jnp.zeros((8, rows), F32)
    squares = jnp.zeros((rows, 128), F32)
    for z in range(own.shape[0]):
        a = own[z].astype(F32)
        b = other[z].astype(F32)
        x = jnp.concatenate([jnp.where(even, a, b), jnp.where(even, b, a)], axis=1)
        squares = squares + x[:, :128] * x[:, :128] + x[:, 128:] * x[:, 128:]
        at = pl.ds(z * 256, 256)
        scaled = (x * gain[:, at]).astype(BF16)
        acc_qk = acc_qk + dot_t(scaled, wqk[:, at])
        acc_vo = acc_vo + dot_t(wvo[:, at], scaled)
        acc_g = acc_g + dot_t(wg[:, at], scaled)
    mean = jnp.sum(squares, axis=1, keepdims=True) * (1.0 / (own.shape[0] * 256))
    inverse = lax.rsqrt(mean + EPS)
    inverse_row = as_row(inverse)
    scale = jnp.where(low_lanes(rows), 1.0, 256.0 ** (-0.5))
    out = acc_qk * inverse * scale
    low = low_lanes(rows)
    extra = []
    for product in (out * norm[...], out * pltpu.roll(out, 64, 1)):
        left = twice(as_row(jnp.sum(jnp.where(low, product, 0.0), axis=1, keepdims=True)))
        for _ in range(3):
            extra.append(left.astype(BF16).astype(F32))
            left = left - extra[-1]
    index = lax.broadcasted_iota(jnp.int32, (16, 128), 0)
    tail = jnp.zeros((16, 128), F32)
    for n, term in enumerate(extra):
        tail = jnp.where(index == n, term, tail)
    out = jnp.concatenate([out, tail], axis=0).astype(BF16)
    for z in range(own.shape[0]):
        payload[z] = out
    acc_vo = acc_vo * inverse_row
    values[...] = acc_vo[:64]
    gates[...] = jax.nn.sigmoid(acc_vo[64:])
    acc_g = acc_g * inverse_row
    ingate = acc_g[:4]
    forget = acc_g[4:] + bias[...]
    logforget = jnp.minimum(forget, 0.0) - jnp.log1p(jnp.exp(-jnp.abs(forget)))
    carried = logforget + state[...]
    top = jnp.maximum(carried, ingate)
    most[...] = top
    floor[...] = jnp.exp(-top)
    decay[...] = jnp.exp(carried - top)
    inflow[...] = jnp.exp(ingate - top)


def twice(x):
    return jnp.concatenate([x, x], axis=1)


def recall_kernel(
    first, own, other, values, gates, floor, decay, inflow, picked, base, state, more, memory, message, keys,
    queries, staged, outgoing, late, out_sems, sems,
):
    heads = 4
    rows = staged.shape[0]
    block = 8
    ready = state.shape[0] + more.shape[0]

    def fetch(i):
        at = pl.ds(i * block, block)
        return pltpu.make_async_copy(memory.at[pl.ds(ready + i * block, block)], late.at[at], sems.at[i])

    start(fetch, late.shape[0] // block)
    even = first[:1, :] == 0
    low = low_lanes(rows)
    for z in range(own.shape[0]):
        a = own[z, :rows].astype(F32)
        b = other[z, :rows].astype(F32)
        e = jnp.where(even, a, b)
        o = jnp.where(even, b, a)
        at = pl.ds(z * 128, 128)
        queries[:, at] = jnp.where(low, e, pltpu.roll(o, 64, 1))
        staged[:, at] = jnp.where(low, pltpu.roll(e, 64, 1), o)
    key_copy = pltpu.make_async_copy(staged, keys, out_sems.at[0])
    key_copy.start()
    lane = lax.broadcasted_iota(jnp.int32, (16, 128), 1) % 64

    ones = jnp.ones((128, 128), BF16)

    def add(source, offset, i, sums):
        block = 4
        sums = list(sums)
        prods = []
        for j in range(block):
            at = i * block + j
            for h in range(heads):
                prod = source[at, h] * queries[pl.ds(offset + at, 1), pl.ds(h * 256, 256)]
                prods.append(prod[:, :128] + prod[:, 128:])
        prods = jnp.concatenate(prods, axis=0)
        high = prods.astype(BF16)
        totals = dot(high, ones) + dot((prods - high.astype(F32)).astype(BF16), ones)
        for j in range(block):
            here = lane == offset + i * block + j
            for h in range(heads):
                at = (j * heads + h) * 16
                sums[h] = jnp.where(here, totals[at : at + 16], sums[h])
        return tuple(sums)

    sums = (jnp.zeros((16, 128), F32),) * heads
    for i in range(state.shape[0] // 4):
        sums = add(state, 0, i, sums)
    for i in range(more.shape[0] // 4):
        sums = add(more, state.shape[0], i, sums)
    kept, fresh = [], []
    for h in range(heads):
        tail = sum(shard[z, rows:].astype(F32) for shard in (own, other) for z in (2 * h, 2 * h + 1))
        nq = tail[0:1] + tail[1:2] + tail[2:3]
        kq = tail[3:4] + tail[4:5] + tail[5:6]
        here = pl.ds(h, 1)
        down, up = twice(decay[here, :]), twice(inflow[here, :])
        bottom = jnp.maximum(jnp.abs(down * nq + up * kq), twice(floor[here, :]))
        kept.append(down / bottom)
        fresh.append(up * kq / bottom)
    for i in range(late.shape[0] // block):
        fetch(i).wait()
        for j in range(block // 4):
            sums = add(late, ready, i * (block // 4) + j, sums)
    half = lax.broadcasted_iota(jnp.int32, (16, 128), 1) < 64
    upper, lower = [], []
    for h in range(heads):
        mine = pl.ds(h * 16, 16)
        gated = twice(gates[mine, :]) * (kept[h] * sums[h] + fresh[h] * twice(values[mine, :]))
        upper.append(jnp.where(half, gated, 0.0))
        lower.append(jnp.where(half, 0.0, gated))
    both = jnp.concatenate(upper + lower, axis=0).astype(BF16)
    sends = []
    for part in range(outgoing.shape[0]):
        out = dot_t(picked[part], both) + base[part].astype(F32)
        outgoing[part] = out.astype(BF16)
        j, c = part // 2, part % 2
        for twin in range(2):
            send = pltpu.make_async_copy(
                outgoing.at[part], message.at[4 * j + 2 * twin + c], out_sems.at[1 + 2 * part + twin]
            )
            send.start()
            sends.append(send)
    for send in sends:
        send.wait()
    key_copy.wait()


def update_kernel(
    decay_scalar, values, decay, inflow, most, keys_hbm, norm_hbm, memory, memory_next, norm_next, most_next,
    keys, norm, norm_out, state, sems, in_sems, out_sems,
):
    heads = 4
    rows = keys.shape[0]
    block = rows // in_sems.shape[0]
    key_copy = pltpu.make_async_copy(keys_hbm, keys, sems.at[0])
    key_copy.start()
    most_copy = pltpu.make_async_copy(most, most_next, sems.at[3])
    most_copy.start()
    fetch = functools.partial(part_copy, memory, state, in_sems)
    send = functools.partial(part_copy, state, memory_next, out_sems)
    start(fetch, in_sems.shape[0])
    norm_copy = pltpu.make_async_copy(norm_hbm, norm, sems.at[1])
    norm_copy.start()
    key_copy.wait()
    lane = lax.broadcasted_iota(jnp.int32, (16, rows), 1)
    fresh = [values[pl.ds(h * 16, 16), :] * inflow[pl.ds(h, 1), :] for h in range(heads)]

    def step(i, carry):
        fetch(i).wait()
        for j in range(block):
            s = i * block + j
            for h in range(heads):
                column = jnp.sum(jnp.where(lane == s, fresh[h], 0.0), axis=1, keepdims=True)
                key = keys[pl.ds(s, 1), pl.ds(h * 256, 256)]
                state[s, h] = decay_scalar[h, s] * state[s, h] + column * key
        send(i).start()
        return carry

    lax.fori_loop(0, in_sems.shape[0], step, 0)
    norm_copy.wait()
    for h in range(heads):
        here = pl.ds(h, 1)
        kept = as_column(decay[here, :])
        norm_out[:, h, :] = kept * norm[:, h, :] + as_column(inflow[here, :]) * keys[:, pl.ds(h * 256, 256)]
    norm_send = pltpu.make_async_copy(norm_out, norm_next, sems.at[2])
    norm_send.start()
    norm_send.wait()
    most_copy.wait()
    drain(send, out_sems.shape[0])


def expert_kernel(
    arrived, gain, staged, mixout, gate_a, gate_b, up_a, up_b, down_a, down_b, out,
    wide, final, weights, downs, sems, weight_sems,
):
    count, groups = arrived.shape[0], arrived.shape[1] // 4

    ready = staged.shape[0]

    def rest(h):
        source = mixout.at[pl.ds(pl.multiple_of(h * 256 + ready * 64, 64), 64)]
        return pltpu.make_async_copy(source, final.at[pl.ds(pl.multiple_of(h * 64, 64), 64)], sems.at[h])

    loads = [
        functools.partial(part_copy, source.at[0], weights.at[n], weight_sems.at[n])
        for n, source in enumerate((gate_a, up_a, gate_b, up_b))
    ]
    loads += [
        functools.partial(part_copy, source.at[0], downs.at[n], weight_sems.at[4 + n])
        for n, source in enumerate((down_a, down_b))
    ]
    for make in [rest] + loads:
        start(make, 4)
    for t in range(count):
        wide[t] = arrived[t].astype(F32)
    low = low_lanes(groups)
    total = jnp.zeros((2 * groups, gain.shape[1]), F32)
    for m in range(count // 4):
        parts, slices = [], []
        for z in range(2):
            t = 4 * m + 2 * z
            e = wide[t, pl.ds(2, groups, stride=4)]
            o = wide[t + 1, pl.ds(2, groups, stride=4)]
            front = jnp.where(low, e, pltpu.roll(o, 64, 1))
            back = jnp.where(low, pltpu.roll(e, 64, 1), o)
            parts.append(jnp.concatenate([front, back], axis=0).astype(BF16))
            slices += [pl.ds(h * 64 + (2 * z + u) * 16, 16) for u in range(2) for h in range(4)]
        if m < ready:
            turned = [staged[m, at, :] for at in slices]
        else:
            drain(rest, 4)
            turned = [final[at, :] for at in slices]
        turned = jnp.concatenate(turned, axis=0)
        total = total + dot(jnp.concatenate(parts, axis=1), turned)
    middle = []
    squares = jnp.zeros((2 * groups, 128), F32)
    for t in range(count):
        rows = [wide[t, pl.ds(b, groups, stride=4)] for b in range(2)]
        piece = jnp.concatenate(rows, axis=0) + total[:, t * 128 : (t + 1) * 128]
        piece = piece.astype(BF16).astype(F32)
        squares = squares + piece * piece
        middle.append(piece)
    mean = jnp.sum(squares, axis=1, keepdims=True) * (1.0 / gain.shape[1])
    inverse = lax.rsqrt(mean + EPS)
    normed = [
        (piece * inverse * gain[:, t * 128 : (t + 1) * 128]).astype(BF16) for t, piece in enumerate(middle)
    ]
    normed = jnp.concatenate(normed, axis=1)
    hidden = []
    for n in range(2):
        drain(loads[2 * n], 4)
        g = dot(normed, weights[2 * n])
        drain(loads[2 * n + 1], 4)
        u = dot(normed, weights[2 * n + 1])
        hidden.append((g * jax.nn.sigmoid(g) * u).astype(BF16))
    part = jnp.zeros((2 * groups, gain.shape[1]), F32)
    for n in range(2):
        drain(loads[4 + n], 4)
        part = part + dot(hidden[n], downs[n])
    for t in range(count):
        piece = part[:, t * 128 : (t + 1) * 128] + 0.5 * middle[t]
        for b in range(2):
            wide[t, pl.ds(b, groups, stride=2)] = piece[b * groups : (b + 1) * groups]
        out[t] = wide[t, : 2 * groups].astype(BF16)


def finish_kernel(returned, columns, out):
    rows, count = columns.shape[0], returned.shape[0]
    q = lax.broadcasted_iota(jnp.int32, (1, count), 1)
    t, g, b = q // 32, (q // 2) % 16, q % 2
    slot = (g * 4 + t // 4) * 4 + 2 * (t % 2) + b
    slot = jnp.broadcast_to(slot.astype(F32), (rows, count))
    total = jnp.zeros((rows, out.shape[1]), F32)
    for k in range(2):
        pick = jnp.where(slot == columns[:, k : k + 1], 1.0, 0.0).astype(BF16)
        total = total + columns[:, 2 + k : 3 + k] * dot(pick, returned[...])
    out[...] = total.astype(BF16)


def local(
    tokens,
    mixer_gain,
    expert_gain,
    query_weight,
    key_weight,
    value_weight,
    outgate_weight,
    ingate_weight,
    forget_weight,
    forget_bias,
    mixout_weight,
    memory_state,
    norm_state,
    max_state,
    expert_gate,
    expert_up,
    expert_down,
    routes,
    route_weights,
):
    rows, own_width = tokens.shape
    width = mixer_gain.shape[0]
    heads, head_dim = norm_state.shape[1:]
    local_values = value_weight.shape[2]
    groups = lax.axis_size("ep")
    tp = lax.axis_size("z") * lax.axis_size("core")
    place = jnp.stack([lax.axis_index("core"), lax.axis_index("z")]).astype(F32)
    place = jnp.broadcast_to(place[:, None], (2, 128))
    z = lax.axis_size("z")
    channels = heads * local_values
    features = heads * head_dim

    own, other = gather_z(jnp.broadcast_to(tokens, (z, rows, own_width)))
    turned = [query_weight.T, key_weight.T]
    turned += [jnp.transpose(w, (1, 2, 0)).reshape(channels, width) for w in (value_weight, outgate_weight)]
    turned += [mixer_gain.reshape(1, width), max_state.T, memory_state]
    small = [routes.T, route_weights.T, tokens, ingate_weight.T, forget_weight.T, norm_state]
    ready, extra = 24, 16
    wqk, wvo, gain, state, loaded, wg, columns, picked, base, norm_own = pl.pallas_call(
        prepare_kernel,
        out_shape=[
            shape((2 * channels, width), BF16),
            shape((2 * channels, width), BF16),
            shape((1, width)),
            shape((heads, rows)),
            shape((ready, *memory_state.shape[1:])),
            shape((2 * heads, width), BF16),
            shape((rows, 128)),
            shape((tp // 2, groups * 4, 128), BF16),
            shape((tp // 2, groups * 4, own_width), BF16),
            shape((rows, 128)),
        ],
        in_specs=[VMEM] + [HBM] * 13,
        out_specs=[VMEM] * 10,
        scratch_shapes=[pltpu.VMEM(x.shape, x.dtype) for x in small]
        + [pltpu.SemaphoreType.DMA((12,)), pltpu.SemaphoreType.DMA((6,))],
        compiler_params=room(6),
        name="prepare",
    )(place, *(hbm(x) for x in small + turned))
    flat = (channels, rows)
    per_head = (heads, rows)
    payload, values, gates, most, floor, decay, inflow = pl.pallas_call(
        project_kernel,
        out_shape=[shape((z, rows + 16, 128), BF16), shape(flat), shape(flat)] + [shape(per_head)] * 4,
        in_specs=[VMEM] * 10,
        out_specs=[VMEM] * 7,
        compiler_params=room(4),
        name="project",
    )(place, own, other, gain, wqk, wvo, wg, forget_bias.reshape(heads, 1), state, norm_own)

    own, other = gather_z(payload)
    more = pl.pallas_call(
        functools.partial(more_kernel, offset=ready),
        out_shape=shape((extra, *memory_state.shape[1:])),
        in_specs=[HBM],
        out_specs=VMEM,
        scratch_shapes=[pltpu.SemaphoreType.DMA((4,))],
        compiler_params=room(4),
        name="more",
    )(hbm(memory_state))
    message, keys = pl.pallas_call(
        recall_kernel,
        out_shape=[pltpu.HBM((tp, groups * 4, own_width), BF16), pltpu.HBM((rows, features), F32)],
        in_specs=[VMEM] * 12 + [HBM],
        out_specs=[HBM] * 2,
        scratch_shapes=[
            pltpu.VMEM((rows, features), F32),
            pltpu.VMEM((rows, features), F32),
            pltpu.VMEM((tp // 2, groups * 4, own_width), BF16),
            pltpu.VMEM((rows - ready - extra, heads, local_values, head_dim), F32),
            pltpu.SemaphoreType.DMA((1 + tp,)),
            pltpu.SemaphoreType.DMA(((rows - ready - extra) // 8,)),
        ],
        compiler_params=room(10),
        name="recall",
    )(
        place, own, other, values, gates, floor, decay, inflow, picked, base, loaded, more,
        hbm(memory_state),
    )
    arrived = exchange(message.reshape(tp * groups, 4, own_width)).reshape(tp, groups * 4, own_width)

    memory_next, norm_next, most = pl.pallas_call(
        update_kernel,
        out_shape=[pltpu.HBM(x.shape, F32) for x in (memory_state, norm_state, most)],
        in_specs=[SMEM] + [VMEM] * 4 + [HBM] * 3,
        out_specs=[HBM] * 3,
        scratch_shapes=[
            pltpu.VMEM(keys.shape, F32),
            pltpu.VMEM(norm_state.shape, F32),
            pltpu.VMEM(norm_state.shape, F32),
            pltpu.VMEM(memory_state.shape, F32),
            pltpu.SemaphoreType.DMA((4,)),
            pltpu.SemaphoreType.DMA((8,)),
            pltpu.SemaphoreType.DMA((8,)),
        ],
        compiler_params=room(8),
        name="update",
    )(decay, values, decay, inflow, most, keys, hbm(norm_state), hbm(memory_state))
    staged = pl.pallas_call(
        stage_kernel,
        out_shape=shape((3, features // 4, width), BF16),
        in_specs=[HBM],
        out_specs=VMEM,
        scratch_shapes=[pltpu.SemaphoreType.DMA((3, 4))],
        compiler_params=room(6),
        name="stage",
    )(hbm(mixout_weight))

    twins = [swap_cores(w) for w in (expert_gate, expert_up, expert_down)]
    pairs = [w for mine, twin in zip((expert_gate, expert_up, expert_down), twins) for w in (mine, twin)]
    part = pl.pallas_call(
        expert_kernel,
        out_shape=shape((tp, groups * 2, own_width), BF16),
        in_specs=[VMEM] * 3 + [HBM] * 7,
        out_specs=VMEM,
        scratch_shapes=[
            pltpu.VMEM((tp, groups * 4, own_width), F32),
            pltpu.VMEM((features // 4, width), BF16),
            pltpu.VMEM((4, *expert_gate.shape[1:]), BF16),
            pltpu.VMEM((2, *expert_down.shape[1:]), BF16),
            pltpu.SemaphoreType.DMA((4,)),
            pltpu.SemaphoreType.DMA((6, 4)),
        ],
        compiler_params=room(16),
        name="expert",
    )(arrived, expert_gain.reshape(1, width), staged, hbm(mixout_weight), *(hbm(w) for w in pairs))
    returned = exchange(part.reshape(tp * groups, 2, own_width)).reshape(tp * groups * 2, own_width)
    mixed_out = pl.pallas_call(
        finish_kernel,
        out_shape=shape((rows, own_width), BF16),
        in_specs=[VMEM] * 2,
        out_specs=VMEM,
        compiler_params=room(4),
        name="finish",
    )(returned, columns)
    return mixed_out, memory_next, norm_next, most.T


def solution(mesh):
    tp = mesh.shape["tp"]
    inner = Mesh(mesh.devices.reshape(mesh.shape["ep"], tp // 2, 2), ("ep", "z", "core"))
    t = ("z", "core")
    every = ("ep", "z", "core")
    in_specs = (
        P("ep", t),
        P(),
        P(),
        P(None, t),
        P(None, t),
        P(None, None, t),
        P(None, None, t),
        P(),
        P(),
        P(),
        P(),
        P("ep", None, t, None),
        P("ep", None, None),
        P("ep", None),
        P(every, None, None),
        P(every, None, None),
        P(every, None, None),
        P("ep", None),
        P("ep", None),
    )
    out_specs = (P("ep", t), P("ep", None, t, None), P("ep", None, None), P("ep", None))
    return jax.shard_map(local, mesh=inner, in_specs=in_specs, out_specs=out_specs, check_vma=False)
```

```python
import functools

import jax
import jax.numpy as jnp
from jax import lax
from jax.experimental import pallas as pl
from jax.experimental.pallas import tpu as pltpu
from jax.sharding import Mesh
from jax.sharding import PartitionSpec as P

EPS = 1e-06
F32 = jnp.float32
BF16 = jnp.bfloat16


def swap_cores(x):
    return lax.ppermute(x, "core", [(0, 1), (1, 0)])


def gather_z(copies):
    own = lax.all_to_all(copies, "z", 0, 0, tiled=True)
    return own, swap_cores(own)


def exchange(x):
    return lax.all_to_all(x, ("z", "core", "ep"), 0, 0, tiled=True)


def hbm(x):
    return pltpu.with_memory_space_constraint(x, pltpu.HBM)


VMEM = pl.BlockSpec(memory_space=pltpu.VMEM)
SMEM = pl.BlockSpec(memory_space=pltpu.SMEM)
HBM = pl.BlockSpec(memory_space=pltpu.HBM)


def room(mib):
    return pltpu.CompilerParams(vmem_limit_bytes=mib * 1024 * 1024)


def shape(dims, dtype=F32):
    return jax.ShapeDtypeStruct(dims, dtype)


def dot(a, b):
    return jnp.dot(a, b, preferred_element_type=F32)


def dot_t(a, b):
    return lax.dot_general(a, b, (((1,), (1,)), ((), ())), preferred_element_type=F32)


def diagonal(n):
    return lax.broadcasted_iota(jnp.int32, (n, n), 0) == lax.broadcasted_iota(jnp.int32, (n, n), 1)


def as_column(row):
    return jnp.sum(jnp.where(diagonal(row.shape[1]), row, 0.0), axis=1, keepdims=True)


def as_row(column):
    return jnp.sum(jnp.where(diagonal(column.shape[0]), column, 0.0), axis=0, keepdims=True)


def low_lanes(rows):
    return lax.broadcasted_iota(jnp.int32, (rows, 128), 1) < 64


def part_copy(source, target, sems, n):
    size = target.shape[0] // sems.shape[0]
    at = pl.ds(pl.multiple_of(n * size, size), size)
    return pltpu.make_async_copy(source.at[at], target.at[at], sems.at[n])


def start(make, count):
    def body(n, carry):
        make(n).start()
        return carry

    lax.fori_loop(0, count, body, 0)


def drain(make, count):
    for n in range(count):
        make(n).wait()


def more_kernel(source, target, sems, *, offset):
    part = functools.partial(part_copy, source.at[pl.ds(offset, target.shape[0])], target, sems)
    start(part, sems.shape[0])
    drain(part, sems.shape[0])


def stage_kernel(mixout, target, sems):
    copies = []
    for m in range(target.shape[0]):
        for h in range(4):
            source = mixout.at[pl.ds(h * 256 + m * 64, 64)]
            copies.append(pltpu.make_async_copy(source, target.at[m, pl.ds(h * 64, 64)], sems.at[m, h]))
    for copy in copies:
        copy.start()
    for copy in copies:
        copy.wait()


def prepare_kernel(
    place, routes_hbm, weights_hbm, tokens_hbm, wi_hbm, wf_hbm, norm_hbm, wq, wk, wv, wo, gain, state, memory,
    wqk, wvo, gain_out, state_out, loaded, wg, columns, picked, base, norm_own,
    routes, weights, tokens, wi, wf, norm, sems, load_sems,
):
    half = wq.shape[0]
    ends = [
        (routes_hbm, routes),
        (weights_hbm, weights),
        (tokens_hbm, tokens),
        (wi_hbm, wi),
        (wf_hbm, wf),
        (norm_hbm, norm),
        (wq, wqk.at[pl.ds(0, half)]),
        (wk, wqk.at[pl.ds(half, half)]),
        (wv, wvo.at[pl.ds(0, half)]),
        (wo, wvo.at[pl.ds(half, half)]),
        (gain, gain_out),
        (state, state_out),
    ]
    copies = [pltpu.make_async_copy(source, target, sems.at[n]) for n, (source, target) in enumerate(ends)]
    for copy in copies:
        copy.start()
    part = functools.partial(part_copy, memory, loaded, load_sems)
    start(part, load_sems.shape[0])
    for copy in copies[:6]:
        copy.wait()
    mine = jnp.zeros(norm_own.shape, F32)
    for z in range(8):
        mine = jnp.where(place[1:2, :] == z, norm[:, z // 2, pl.ds((z % 2) * 128, 128)], mine)
    norm_own[...] = jnp.where(place[:1, :] == 0, mine, pltpu.roll(mine, 64, 1))
    wg[...] = jnp.concatenate([wi[...].astype(F32), wf[...].astype(F32)], axis=0).astype(BF16)
    count = tokens.shape[0]
    at_row = lax.broadcasted_iota(jnp.int32, (count, count), 0)
    at_column = lax.broadcasted_iota(jnp.int32, (count, count), 1)
    experts = [as_column(routes[k : k + 1, :].astype(F32)) for k in range(2)]
    named = [(expert == at_column.astype(F32)).astype(F32) for expert in experts]
    earlier = (at_column < at_row).astype(F32)
    counts = dot(earlier.astype(BF16), (named[0] + named[1]).astype(BF16))
    total = weights[:1, :] + weights[1:, :]
    lane = lax.broadcasted_iota(jnp.int32, (count, 128), 1)
    out = jnp.zeros((count, 128), F32)
    targets = []
    for k in range(2):
        rank = jnp.sum(counts * named[k], axis=1, keepdims=True)
        target = experts[k] * 4.0 + rank
        out = jnp.where(lane == k, target, out)
        out = jnp.where(lane == 2 + k, as_column(weights[k : k + 1, :] / total), out)
        targets.append(twice(as_row(target)))
    columns[...] = out
    rows = picked.shape[1]
    row = lax.broadcasted_iota(jnp.int32, (rows, 128), 0)
    kind = lax.broadcasted_iota(jnp.int32, (rows, 128), 1) // 64
    r = row % 4
    for n in range(picked.shape[0]):
        first = (row // 4) * 16 + 2 * n
        slot = jnp.where(r == 2, first + kind, -1).astype(F32)
        picked[n] = jnp.where((slot == targets[0]) | (slot == targets[1]), 1.0, 0.0).astype(BF16)
        slot = jnp.where(r < 2, first + r, -1).astype(F32)
        chosen = jnp.where((slot == targets[0]) | (slot == targets[1]), 1.0, 0.0)
        base[n] = dot(chosen[:, :64].astype(BF16), tokens[...]).astype(BF16)
    for copy in copies[6:]:
        copy.wait()
    drain(part, load_sems.shape[0])


def project_kernel(
    first, own, other, gain, wqk, wvo, wg, bias, state, norm, payload, values, gates, most, floor, decay, inflow
):
    even = first[:1, :] == 0
    rows = own.shape[1]
    acc_qk = jnp.zeros((rows, 128), F32)
    acc_vo = jnp.zeros((128, rows), F32)
    acc_g = jnp.zeros((8, rows), F32)
    squares = jnp.zeros((rows, 128), F32)
    for z in range(own.shape[0]):
        a = own[z].astype(F32)
        b = other[z].astype(F32)
        x = jnp.concatenate([jnp.where(even, a, b), jnp.where(even, b, a)], axis=1)
        squares = squares + x[:, :128] * x[:, :128] + x[:, 128:] * x[:, 128:]
        at = pl.ds(z * 256, 256)
        scaled = (x * gain[:, at]).astype(BF16)
        acc_qk = acc_qk + dot_t(scaled, wqk[:, at])
        acc_vo = acc_vo + dot_t(wvo[:, at], scaled)
        acc_g = acc_g + dot_t(wg[:, at], scaled)
    mean = jnp.sum(squares, axis=1, keepdims=True) * (1.0 / (own.shape[0] * 256))
    inverse = lax.rsqrt(mean + EPS)
    inverse_row = as_row(inverse)
    scale = jnp.where(low_lanes(rows), 1.0, 256.0 ** (-0.5))
    out = acc_qk * inverse * scale
    low = low_lanes(rows)
    extra = []
    for product in (out * norm[...], out * pltpu.roll(out, 64, 1)):
        left = twice(as_row(jnp.sum(jnp.where(low, product, 0.0), axis=1, keepdims=True)))
        for _ in range(3):
            extra.append(left.astype(BF16).astype(F32))
            left = left - extra[-1]
    index = lax.broadcasted_iota(jnp.int32, (16, 128), 0)
    tail = jnp.zeros((16, 128), F32)
    for n, term in enumerate(extra):
        tail = jnp.where(index == n, term, tail)
    out = jnp.concatenate([out, tail], axis=0).astype(BF16)
    for z in range(own.shape[0]):
        payload[z] = out
    acc_vo = acc_vo * inverse_row
    values[...] = acc_vo[:64]
    gates[...] = jax.nn.sigmoid(acc_vo[64:])
    acc_g = acc_g * inverse_row
    ingate = acc_g[:4]
    forget = acc_g[4:] + bias[...]
    logforget = jnp.minimum(forget, 0.0) - jnp.log1p(jnp.exp(-jnp.abs(forget)))
    carried = logforget + state[...]
    top = jnp.maximum(carried, ingate)
    most[...] = top
    floor[...] = jnp.exp(-top)
    decay[...] = jnp.exp(carried - top)
    inflow[...] = jnp.exp(ingate - top)


def twice(x):
    return jnp.concatenate([x, x], axis=1)


def recall_kernel(
    first, own, other, values, gates, floor, decay, inflow, picked, base, state, more, memory, message, keys,
    queries, staged, outgoing, late, out_sems, sems,
):
    heads = 4
    rows = staged.shape[0]
    block = 8
    ready = state.shape[0] + more.shape[0]

    def fetch(i):
        at = pl.ds(i * block, block)
        return pltpu.make_async_copy(memory.at[pl.ds(ready + i * block, block)], late.at[at], sems.at[i])

    start(fetch, late.shape[0] // block)
    even = first[:1, :] == 0
    low = low_lanes(rows)
    for z in range(own.shape[0]):
        a = own[z, :rows].astype(F32)
        b = other[z, :rows].astype(F32)
        e = jnp.where(even, a, b)
        o = jnp.where(even, b, a)
        at = pl.ds(z * 128, 128)
        queries[:, at] = jnp.where(low, e, pltpu.roll(o, 64, 1))
        staged[:, at] = jnp.where(low, pltpu.roll(e, 64, 1), o)
    key_copy = pltpu.make_async_copy(staged, keys, out_sems.at[0])
    key_copy.start()
    lane = lax.broadcasted_iota(jnp.int32, (16, 128), 1) % 64

    ones = jnp.ones((128, 128), BF16)

    def add(source, offset, i, sums):
        block = 4
        sums = list(sums)
        prods = []
        for j in range(block):
            at = i * block + j
            for h in range(heads):
                prod = source[at, h] * queries[pl.ds(offset + at, 1), pl.ds(h * 256, 256)]
                prods.append(prod[:, :128] + prod[:, 128:])
        prods = jnp.concatenate(prods, axis=0)
        high = prods.astype(BF16)
        totals = dot(high, ones) + dot((prods - high.astype(F32)).astype(BF16), ones)
        for j in range(block):
            here = lane == offset + i * block + j
            for h in range(heads):
                at = (j * heads + h) * 16
                sums[h] = jnp.where(here, totals[at : at + 16], sums[h])
        return tuple(sums)

    sums = (jnp.zeros((16, 128), F32),) * heads
    for i in range(state.shape[0] // 4):
        sums = add(state, 0, i, sums)
    for i in range(more.shape[0] // 4):
        sums = add(more, state.shape[0], i, sums)
    kept, fresh, bottoms = [], [], []
    for h in range(heads):
        tail = sum(shard[z, rows:].astype(F32) for shard in (own, other) for z in (2 * h, 2 * h + 1))
        nq = tail[0:1] + tail[1:2] + tail[2:3]
        kq = tail[3:4] + tail[4:5] + tail[5:6]
        here = pl.ds(h, 1)
        down, up = twice(decay[here, :]), twice(inflow[here, :])
        bottom = jnp.maximum(jnp.abs(down * nq + up * kq), twice(floor[here, :]))
        kept.append(down)
        fresh.append(up * kq)
        bottoms.append(bottom)
    for i in range(late.shape[0] // block):
        fetch(i).wait()
        for j in range(block // 4):
            sums = add(late, ready, i * (block // 4) + j, sums)
    half = lax.broadcasted_iota(jnp.int32, (16, 128), 1) < 64
    upper, lower = [], []
    for h in range(heads):
        mine = pl.ds(h * 16, 16)
        number = kept[h] * sums[h] + fresh[h] * twice(values[mine, :])
        gated = twice(gates[mine, :]) * (number / bottoms[h])
        upper.append(jnp.where(half, gated, 0.0))
        lower.append(jnp.where(half, 0.0, gated))
    both = jnp.concatenate(upper + lower, axis=0).astype(BF16)
    sends = []
    for part in range(outgoing.shape[0]):
        out = dot_t(picked[part], both) + base[part].astype(F32)
        outgoing[part] = out.astype(BF16)
        j, c = part // 2, part % 2
        for twin in range(2):
            send = pltpu.make_async_copy(
                outgoing.at[part], message.at[4 * j + 2 * twin + c], out_sems.at[1 + 2 * part + twin]
            )
            send.start()
            sends.append(send)
    for send in sends:
        send.wait()
    key_copy.wait()


def update_kernel(
    decay_scalar, values, decay, inflow, most, keys_hbm, norm_hbm, memory, memory_next, norm_next, most_next,
    keys, norm, norm_out, state, sems, in_sems, out_sems,
):
    heads = 4
    rows = keys.shape[0]
    block = rows // in_sems.shape[0]
    key_copy = pltpu.make_async_copy(keys_hbm, keys, sems.at[0])
    key_copy.start()
    most_copy = pltpu.make_async_copy(most, most_next, sems.at[3])
    most_copy.start()
    fetch = functools.partial(part_copy, memory, state, in_sems)
    send = functools.partial(part_copy, state, memory_next, out_sems)
    start(fetch, in_sems.shape[0])
    norm_copy = pltpu.make_async_copy(norm_hbm, norm, sems.at[1])
    norm_copy.start()
    key_copy.wait()
    lane = lax.broadcasted_iota(jnp.int32, (16, rows), 1)
    fresh = [values[pl.ds(h * 16, 16), :] * inflow[pl.ds(h, 1), :] for h in range(heads)]

    def step(i, carry):
        fetch(i).wait()
        for j in range(block):
            s = i * block + j
            for h in range(heads):
                column = jnp.sum(jnp.where(lane == s, fresh[h], 0.0), axis=1, keepdims=True)
                key = keys[pl.ds(s, 1), pl.ds(h * 256, 256)]
                state[s, h] = decay_scalar[h, s] * state[s, h] + column * key
        send(i).start()
        return carry

    lax.fori_loop(0, in_sems.shape[0], step, 0)
    norm_copy.wait()
    for h in range(heads):
        here = pl.ds(h, 1)
        kept = as_column(decay[here, :])
        norm_out[:, h, :] = kept * norm[:, h, :] + as_column(inflow[here, :]) * keys[:, pl.ds(h * 256, 256)]
    norm_send = pltpu.make_async_copy(norm_out, norm_next, sems.at[2])
    norm_send.start()
    norm_send.wait()
    most_copy.wait()
    drain(send, out_sems.shape[0])


def expert_kernel(
    arrived, gain, staged, mixout, gate_a, gate_b, up_a, up_b, down_a, down_b, out,
    wide, final, weights, downs, sems, weight_sems,
):
    count, groups = arrived.shape[0], arrived.shape[1] // 4

    ready = staged.shape[0]

    def rest(h):
        source = mixout.at[pl.ds(pl.multiple_of(h * 256 + ready * 64, 64), 64)]
        return pltpu.make_async_copy(source, final.at[pl.ds(pl.multiple_of(h * 64, 64), 64)], sems.at[h])

    loads = [
        functools.partial(part_copy, source.at[0], weights.at[n], weight_sems.at[n])
        for n, source in enumerate((gate_a, up_a, gate_b, up_b))
    ]
    loads += [
        functools.partial(part_copy, source.at[0], downs.at[n], weight_sems.at[4 + n])
        for n, source in enumerate((down_a, down_b))
    ]
    for make in [rest] + loads:
        start(make, 4)
    for t in range(count):
        wide[t] = arrived[t].astype(F32)
    low = low_lanes(groups)
    total = jnp.zeros((2 * groups, gain.shape[1]), F32)
    for m in range(count // 4):
        parts, slices = [], []
        for z in range(2):
            t = 4 * m + 2 * z
            e = wide[t, pl.ds(2, groups, stride=4)]
            o = wide[t + 1, pl.ds(2, groups, stride=4)]
            front = jnp.where(low, e, pltpu.roll(o, 64, 1))
            back = jnp.where(low, pltpu.roll(e, 64, 1), o)
            parts.append(jnp.concatenate([front, back], axis=0).astype(BF16))
            slices += [pl.ds(h * 64 + (2 * z + u) * 16, 16) for u in range(2) for h in range(4)]
        if m < ready:
            turned = [staged[m, at, :] for at in slices]
        else:
            drain(rest, 4)
            turned = [final[at, :] for at in slices]
        turned = jnp.concatenate(turned, axis=0)
        total = total + dot(jnp.concatenate(parts, axis=1), turned)
    middle = []
    squares = jnp.zeros((2 * groups, 128), F32)
    for t in range(count):
        rows = [wide[t, pl.ds(b, groups, stride=4)] for b in range(2)]
        piece = jnp.concatenate(rows, axis=0) + total[:, t * 128 : (t + 1) * 128]
        piece = piece.astype(BF16).astype(F32)
        squares = squares + piece * piece
        middle.append(piece)
    mean = jnp.sum(squares, axis=1, keepdims=True) * (1.0 / gain.shape[1])
    inverse = lax.rsqrt(mean + EPS)
    normed = [
        (piece * inverse * gain[:, t * 128 : (t + 1) * 128]).astype(BF16) for t, piece in enumerate(middle)
    ]
    normed = jnp.concatenate(normed, axis=1)
    hidden = []
    for n in range(2):
        drain(loads[2 * n], 4)
        g = dot(normed, weights[2 * n])
        drain(loads[2 * n + 1], 4)
        u = dot(normed, weights[2 * n + 1])
        hidden.append((g * jax.nn.sigmoid(g) * u).astype(BF16))
    part = jnp.zeros((2 * groups, gain.shape[1]), F32)
    for n in range(2):
        drain(loads[4 + n], 4)
        part = part + dot(hidden[n], downs[n])
    for t in range(count):
        piece = part[:, t * 128 : (t + 1) * 128] + 0.5 * middle[t]
        for b in range(2):
            wide[t, pl.ds(b, groups, stride=2)] = piece[b * groups : (b + 1) * groups]
        out[t] = wide[t, : 2 * groups].astype(BF16)


def finish_kernel(returned, columns, out):
    rows, count = columns.shape[0], returned.shape[0]
    q = lax.broadcasted_iota(jnp.int32, (1, count), 1)
    t, g, b = q // 32, (q // 2) % 16, q % 2
    slot = (g * 4 + t // 4) * 4 + 2 * (t % 2) + b
    slot = jnp.broadcast_to(slot.astype(F32), (rows, count))
    total = jnp.zeros((rows, out.shape[1]), F32)
    for k in range(2):
        pick = jnp.where(slot == columns[:, k : k + 1], 1.0, 0.0).astype(BF16)
        total = total + columns[:, 2 + k : 3 + k] * dot(pick, returned[...])
    out[...] = total.astype(BF16)


def local(
    tokens,
    mixer_gain,
    expert_gain,
    query_weight,
    key_weight,
    value_weight,
    outgate_weight,
    ingate_weight,
    forget_weight,
    forget_bias,
    mixout_weight,
    memory_state,
    norm_state,
    max_state,
    expert_gate,
    expert_up,
    expert_down,
    routes,
    route_weights,
):
    rows, own_width = tokens.shape
    width = mixer_gain.shape[0]
    heads, head_dim = norm_state.shape[1:]
    local_values = value_weight.shape[2]
    groups = lax.axis_size("ep")
    tp = lax.axis_size("z") * lax.axis_size("core")
    place = jnp.stack([lax.axis_index("core"), lax.axis_index("z")]).astype(F32)
    place = jnp.broadcast_to(place[:, None], (2, 128))
    z = lax.axis_size("z")
    channels = heads * local_values
    features = heads * head_dim

    own, other = gather_z(jnp.broadcast_to(tokens, (z, rows, own_width)))
    turned = [query_weight.T, key_weight.T]
    turned += [jnp.transpose(w, (1, 2, 0)).reshape(channels, width) for w in (value_weight, outgate_weight)]
    turned += [mixer_gain.reshape(1, width), max_state.T, memory_state]
    small = [routes.T, route_weights.T, tokens, ingate_weight.T, forget_weight.T, norm_state]
    ready, extra = 24, 16
    wqk, wvo, gain, state, loaded, wg, columns, picked, base, norm_own = pl.pallas_call(
        prepare_kernel,
        out_shape=[
            shape((2 * channels, width), BF16),
            shape((2 * channels, width), BF16),
            shape((1, width)),
            shape((heads, rows)),
            shape((ready, *memory_state.shape[1:])),
            shape((2 * heads, width), BF16),
            shape((rows, 128)),
            shape((tp // 2, groups * 4, 128), BF16),
            shape((tp // 2, groups * 4, own_width), BF16),
            shape((rows, 128)),
        ],
        in_specs=[VMEM] + [HBM] * 13,
        out_specs=[VMEM] * 10,
        scratch_shapes=[pltpu.VMEM(x.shape, x.dtype) for x in small]
        + [pltpu.SemaphoreType.DMA((12,)), pltpu.SemaphoreType.DMA((6,))],
        compiler_params=room(6),
        name="prepare",
    )(place, *(hbm(x) for x in small + turned))
    flat = (channels, rows)
    per_head = (heads, rows)
    payload, values, gates, most, floor, decay, inflow = pl.pallas_call(
        project_kernel,
        out_shape=[shape((z, rows + 16, 128), BF16), shape(flat), shape(flat)] + [shape(per_head)] * 4,
        in_specs=[VMEM] * 10,
        out_specs=[VMEM] * 7,
        compiler_params=room(4),
        name="project",
    )(place, own, other, gain, wqk, wvo, wg, forget_bias.reshape(heads, 1), state, norm_own)

    own, other = gather_z(payload)
    more = pl.pallas_call(
        functools.partial(more_kernel, offset=ready),
        out_shape=shape((extra, *memory_state.shape[1:])),
        in_specs=[HBM],
        out_specs=VMEM,
        scratch_shapes=[pltpu.SemaphoreType.DMA((4,))],
        compiler_params=room(4),
        name="more",
    )(hbm(memory_state))
    message, keys = pl.pallas_call(
        recall_kernel,
        out_shape=[pltpu.HBM((tp, groups * 4, own_width), BF16), pltpu.HBM((rows, features), F32)],
        in_specs=[VMEM] * 12 + [HBM],
        out_specs=[HBM] * 2,
        scratch_shapes=[
            pltpu.VMEM((rows, features), F32),
            pltpu.VMEM((rows, features), F32),
            pltpu.VMEM((tp // 2, groups * 4, own_width), BF16),
            pltpu.VMEM((rows - ready - extra, heads, local_values, head_dim), F32),
            pltpu.SemaphoreType.DMA((1 + tp,)),
            pltpu.SemaphoreType.DMA(((rows - ready - extra) // 8,)),
        ],
        compiler_params=room(10),
        name="recall",
    )(
        place, own, other, values, gates, floor, decay, inflow, picked, base, loaded, more,
        hbm(memory_state),
    )
    arrived = exchange(message.reshape(tp * groups, 4, own_width)).reshape(tp, groups * 4, own_width)

    memory_next, norm_next, most = pl.pallas_call(
        update_kernel,
        out_shape=[pltpu.HBM(x.shape, F32) for x in (memory_state, norm_state, most)],
        in_specs=[SMEM] + [VMEM] * 4 + [HBM] * 3,
        out_specs=[HBM] * 3,
        scratch_shapes=[
            pltpu.VMEM(keys.shape, F32),
            pltpu.VMEM(norm_state.shape, F32),
            pltpu.VMEM(norm_state.shape, F32),
            pltpu.VMEM(memory_state.shape, F32),
            pltpu.SemaphoreType.DMA((4,)),
            pltpu.SemaphoreType.DMA((8,)),
            pltpu.SemaphoreType.DMA((8,)),
        ],
        compiler_params=room(8),
        name="update",
    )(decay, values, decay, inflow, most, keys, hbm(norm_state), hbm(memory_state))
    staged = pl.pallas_call(
        stage_kernel,
        out_shape=shape((3, features // 4, width), BF16),
        in_specs=[HBM],
        out_specs=VMEM,
        scratch_shapes=[pltpu.SemaphoreType.DMA((3, 4))],
        compiler_params=room(6),
        name="stage",
    )(hbm(mixout_weight))

    twins = [swap_cores(w) for w in (expert_gate, expert_up, expert_down)]
    pairs = [w for mine, twin in zip((expert_gate, expert_up, expert_down), twins) for w in (mine, twin)]
    part = pl.pallas_call(
        expert_kernel,
        out_shape=shape((tp, groups * 2, own_width), BF16),
        in_specs=[VMEM] * 3 + [HBM] * 7,
        out_specs=VMEM,
        scratch_shapes=[
            pltpu.VMEM((tp, groups * 4, own_width), F32),
            pltpu.VMEM((features // 4, width), BF16),
            pltpu.VMEM((4, *expert_gate.shape[1:]), BF16),
            pltpu.VMEM((2, *expert_down.shape[1:]), BF16),
            pltpu.SemaphoreType.DMA((4,)),
            pltpu.SemaphoreType.DMA((6, 4)),
        ],
        compiler_params=room(16),
        name="expert",
    )(arrived, expert_gain.reshape(1, width), staged, hbm(mixout_weight), *(hbm(w) for w in pairs))
    returned = exchange(part.reshape(tp * groups, 2, own_width)).reshape(tp * groups * 2, own_width)
    mixed_out = pl.pallas_call(
        finish_kernel,
        out_shape=shape((rows, own_width), BF16),
        in_specs=[VMEM] * 2,
        out_specs=VMEM,
        compiler_params=room(4),
        name="finish",
    )(returned, columns)
    return mixed_out, memory_next, norm_next, most.T


def solution(mesh):
    tp = mesh.shape["tp"]
    inner = Mesh(mesh.devices.reshape(mesh.shape["ep"], tp // 2, 2), ("ep", "z", "core"))
    t = ("z", "core")
    every = ("ep", "z", "core")
    in_specs = (
        P("ep", t),
        P(),
        P(),
        P(None, t),
        P(None, t),
        P(None, None, t),
        P(None, None, t),
        P(),
        P(),
        P(),
        P(),
        P("ep", None, t, None),
        P("ep", None, None),
        P("ep", None),
        P(every, None, None),
        P(every, None, None),
        P(every, None, None),
        P("ep", None),
        P("ep", None),
    )
    out_specs = (P("ep", t), P("ep", None, t, None), P("ep", None, None), P("ep", None))
    return jax.shard_map(local, mesh=inner, in_specs=in_specs, out_specs=out_specs, check_vma=False)
```
